32 devices in a mesh: dp: 4 (over y, x), kv: 4 (over z), tp: 2 (over core).
Axes of the slice: x: 2, y: 2, z: 4, core: 2. Of those that a mesh axis runs over, the one named last changes fastest.
Arguments:
- tokens: bfloat16 [32, 4096], P('dp', ('kv', 'tp')), as said below
- query_weight: bfloat16 [4096, 16, 128], P(None, 'tp', 'kv'), may hold values from -0.09375 to 0.09375
- key_weight: bfloat16 [4096, 16, 128], P(None, 'tp', 'kv'), may hold values from -0.09375 to 0.09375
- value_weight: bfloat16 [4096, 16, 256], P(None, 'tp', 'kv'), may hold values from -0.09375 to 0.09375
- gate_weight: bfloat16 [4096, 16, 256], P(None, 'tp', 'kv'), may hold values from -0.09375 to 0.09375
- decay_weight: bfloat16 [4096, 16, 128], P(None, 'tp', 'kv'), may hold values from -0.09375 to 0.09375
- decay_bias: float32 [16, 128], P('tp'), may hold values from -8 to 2
- states: float32 [32, 16, 128, 256], P(('dp', 'kv'), 'tp'), may hold values from -4 to 4
- head_gain: float32 [16, 256], P('tp'), may hold values from 0.1 to 1.9
- out_weight: bfloat16 [4096, 4096], P(None, ('kv', 'tp')), as said below
- norm1_gain: float32 [4096], P(('kv', 'tp')), may hold values from 0.1 to 1.9
- norm1_bias: float32 [4096], P(('kv', 'tp')), may hold values from -3 to 3
- up_weight: bfloat16 [4096, 16384], P(None, ('kv', 'tp')), may hold values from -0.09375 to 0.09375
- down_weight: bfloat16 [16384, 4096], P(('kv', 'tp')), as said below
- norm2_gain: float32 [4096], P(('kv', 'tp')), may hold values from 0.1 to 1.9
- norm2_bias: float32 [4096], P(('kv', 'tp')), may hold values from -3 to 3
Outputs:
- layer_out: bfloat16 [32, 4096], P('dp', ('kv', 'tp'))
- new_states: float32 [32, 16, 128, 256], P(('dp', 'kv'), 'tp')
The draws below stay inside these ranges and needn't reach their ends.
Inputs may be any that keep to these rules, and one draw needn't show every extreme that they name: `tokens`: each block of 64 features has its own scale. `out_weight`: entries lie within 13 / sqrt(4096) of zero. `down_weight`: entries lie within 14 / sqrt(16384) of zero.
All inputs are finite; a program needn't handle non-finite values.
Results may differ from the reference program's by a relative error of at most 0.009.
Values may be sent and summed in bfloat16 or wider, within the bound.
A program may use at most 128 MiB of HBM per device.

```python
import jax
import jax.numpy as jnp
from jax import lax

D = 4096
HEADS = 16
KEY_DIM = 128
VALUE_DIM = 256
MIXER_UNITS = 16384
ROWS = 32


def draw_tokens(key, part):
    base_key, scale_key = jax.random.split(key, 2)
    column_scale = jnp.exp(jax.random.uniform(scale_key, (D // 64,), jnp.float32, -1.0, 1.0))
    column_scale = jnp.repeat(column_scale, 64)
    values = jax.random.normal(base_key, (ROWS, D), jnp.float32)
    return (values * column_scale).astype(jnp.bfloat16)


def draw_out_weight(key, part):
    noise_key, left_key, right_key = jax.random.split(jax.random.fold_in(key, 31), 3)
    fan_in = HEADS * VALUE_DIM
    left = jnp.clip(jax.random.normal(left_key, (fan_in, 1), jnp.float32), -3.0, 3.0)
    right = jnp.clip(jax.random.normal(right_key, (1, D), jnp.float32), -3.0, 3.0)
    noise = jnp.clip(jax.random.normal(noise_key, (fan_in, D), jnp.float32), -6.0, 6.0)
    common = 0.8 * left * right
    return ((0.6 * noise + common) * fan_in ** (-0.5)).astype(jnp.bfloat16)


def draw_down_weight(key, part):
    noise_key, offset_key = jax.random.split(jax.random.fold_in(key, 47), 2)
    noise = jnp.clip(jax.random.normal(noise_key, (MIXER_UNITS, D), jnp.float32), -6.0, 6.0)
    offset = jax.random.uniform(offset_key, (1, D), jnp.float32, -5.0, 5.0)
    values = noise * MIXER_UNITS ** (-0.5) + offset / MIXER_UNITS
    return values.astype(jnp.bfloat16)


def block_levels(own_key, dims, shards, low, top_value):
    level, own = 1.0, jax.random.fold_in(own_key, 6)
    for dim, blocks in shards:
        steps = jnp.exp(jax.random.uniform(jax.random.fold_in(own, dim), (blocks,), jnp.float32, low / len(shards), top_value / len(shards)))
        level = level * jnp.repeat(steps, dims[dim] // blocks).reshape([-1 if axis == dim else 1 for axis in range(len(dims))])
    return level


def scatter_about(stream_key, shape, scale, reach, cuts=(), kind=jnp.bfloat16):
    values = scale * jax.random.normal(stream_key, shape, jnp.float32)
    if cuts:
        values = values * block_levels(stream_key, shape, cuts, -0.22, 0.18)
    return jnp.clip(values, -reach, reach).astype(kind)


def setup_inputs(seed: int = 0) -> dict:
    keys = jax.random.split(jax.random.key(seed), 17)
    return {
        "tokens": draw_tokens(jax.random.fold_in(keys[16], 71), 0),
        "query_weight": scatter_about(keys[1], (D, HEADS, KEY_DIM), D ** -0.5, 0.09375, ((1, 2), (2, 4))),
        "key_weight": scatter_about(keys[2], (D, HEADS, KEY_DIM), D ** -0.5, 0.09375, ((1, 2), (2, 4))),
        "value_weight": scatter_about(keys[3], (D, HEADS, VALUE_DIM), D ** -0.5, 0.09375, ((1, 2), (2, 4))),
        "gate_weight": scatter_about(keys[4], (D, HEADS, VALUE_DIM), D ** -0.5, 0.09375, ((1, 2), (2, 4))),
        "decay_weight": scatter_about(keys[5], (D, HEADS, KEY_DIM), D ** -0.5, 0.09375, ((1, 2), (2, 4))),
        "decay_bias": jnp.clip(-8.0 + 10.0 * jax.random.uniform(keys[6], (HEADS, KEY_DIM), jnp.float32) ** block_levels(keys[6], (HEADS, KEY_DIM), ((0, 2),), -0.2, 0.2), -8.0, 2.0),
        "states": scatter_about(keys[7], (ROWS, HEADS, KEY_DIM, VALUE_DIM), 0.5, 4.0, ((0, 16), (1, 2)), jnp.float32),
        "head_gain": jnp.clip(1.0 + 0.18 * jax.random.normal(keys[8], (HEADS, VALUE_DIM), jnp.float32), 0.1, 1.9),
        "out_weight": draw_out_weight(jax.random.fold_in(keys[16], 71), 0),
        "norm1_gain": jnp.clip(1.0 + 0.18 * jax.random.normal(keys[10], (D,), jnp.float32), 0.1, 1.9),
        "norm1_bias": scatter_about(keys[11], (D,), 0.5, 3.0, ((0, 8),), jnp.float32),
        "up_weight": scatter_about(keys[12], (D, MIXER_UNITS), D ** -0.5, 0.09375, ((1, 8),)),
        "down_weight": draw_down_weight(jax.random.fold_in(keys[16], 71), 0),
        "norm2_gain": jnp.clip(1.0 + 0.18 * jax.random.normal(keys[14], (D,), jnp.float32), 0.1, 1.9),
        "norm2_bias": scatter_about(keys[15], (D,), 0.5, 3.0, ((0, 8),), jnp.float32),
    }


ALPHA = 2.0 ** 0.5
TAU = 16.0
LN_EPS = 1e-05
RMS_EPS = 1e-06

def project(inputs, weight):
    flattened = weight.reshape(weight.shape[0], -1)
    return jnp.dot(inputs, flattened, preferred_element_type=jnp.float32).astype(jnp.bfloat16)

def normalize(inputs, row_gain, row_shift):
    average = lax.optimization_barrier(jnp.sum(inputs, axis=-1, keepdims=True)) / inputs.shape[-1]
    spread = lax.optimization_barrier(jnp.sum(inputs * inputs, axis=-1, keepdims=True)) / inputs.shape[-1] - average * average
    return ((inputs - average) * lax.rsqrt(spread + LN_EPS) * row_gain + row_shift).astype(jnp.bfloat16)

def reference(tokens, query_weight, key_weight, value_weight, gate_weight, decay_weight, decay_bias, states, head_gain, out_weight, norm1_gain, norm1_bias, up_weight, down_weight, norm2_gain, norm2_bias):
    row_count = tokens.shape[0]
    query_rows = project(tokens, query_weight).astype(jnp.float32).reshape(row_count, HEADS, KEY_DIM) * KEY_DIM ** (-0.5)
    key_rows = project(tokens, key_weight).astype(jnp.float32).reshape(row_count, HEADS, KEY_DIM)
    decay_rows = project(tokens, decay_weight).astype(jnp.float32).reshape(row_count, HEADS, KEY_DIM)
    value_rows = project(tokens, value_weight).astype(jnp.float32).reshape(row_count, HEADS, VALUE_DIM)
    gate_rows = project(tokens, gate_weight).astype(jnp.float32).reshape(row_count, HEADS, VALUE_DIM)
    retain = jnp.exp(jax.nn.log_sigmoid(decay_rows + decay_bias) / TAU)
    new_states = retain[..., None] * states + key_rows[..., :, None] * value_rows[..., None, :]
    readout = jnp.einsum('rhk,rhkv->rhv', query_rows, new_states, precision=lax.Precision.HIGHEST)
    readout = readout * lax.rsqrt(lax.optimization_barrier(jnp.mean(readout * readout, axis=-1, keepdims=True)) + RMS_EPS) * head_gain
    attended = (readout * jax.nn.silu(gate_rows)).astype(jnp.bfloat16).reshape(row_count, HEADS * VALUE_DIM)
    mixed_heads = jnp.dot(attended, out_weight, preferred_element_type=jnp.float32)
    residual_one = ALPHA * tokens.astype(jnp.float32) + mixed_heads
    normed = normalize(residual_one, norm1_gain, norm1_bias)
    lifted = jnp.dot(normed, up_weight, preferred_element_type=jnp.float32)
    hidden = jnp.square(jax.nn.relu(lifted)).astype(jnp.bfloat16)
    residual_two = ALPHA * normed.astype(jnp.float32) + jnp.dot(hidden, down_weight, preferred_element_type=jnp.float32)
    return (normalize(residual_two, norm2_gain, norm2_bias), new_states)
```

```python
import functools

import jax
import jax.numpy as jnp
from jax import lax
from jax.experimental import pallas as pl
from jax.experimental.pallas import tpu as pltpu
from jax.sharding import PartitionSpec as P

D = 4096
KEY_DIM = 128


ALPHA = 2.0**0.5
TAU = 16.0
LN_EPS = 1e-05
RMS_EPS = 1e-06


def project_flat(inputs, weight):
    flattened = weight.reshape(weight.shape[0], -1)
    return jnp.dot(inputs, flattened, preferred_element_type=jnp.float32).astype(jnp.bfloat16)


def normalize(inputs, average, spread, row_gain, row_shift):
    return ((inputs - average) * lax.rsqrt(spread + LN_EPS) * row_gain + row_shift).astype(
        jnp.bfloat16
    )


def body(
    tokens,
    query_weight,
    key_weight,
    value_weight,
    gate_weight,
    decay_weight,
    decay_bias,
    states,
    head_gain,
    out_weight,
    norm1_gain,
    norm1_bias,
    up_weight,
    down_weight,
    norm2_gain,
    norm2_bias,
):
    whole = lax.all_gather(tokens, ("kv", "tp"), axis=1, tiled=True)
    weights_list = (query_weight, key_weight, decay_weight, value_weight, gate_weight)
    packed = jnp.concatenate([project_flat(whole, weight) for weight in weights_list], axis=1)
    arrived = lax.all_to_all(packed, "kv", split_axis=0, concat_axis=0, tiled=True)
    groups = lax.axis_size("kv")
    seq_count = whole.shape[0] // groups
    local_heads = query_weight.shape[1]
    unpacked = []
    start = 0
    for weight in weights_list:
        channels = weight.shape[2]
        width = local_heads * channels
        block = arrived[:, start : start + width].reshape(groups, seq_count, local_heads, channels)
        block = block.transpose(1, 2, 0, 3).reshape(seq_count, local_heads, groups * channels)
        unpacked.append(block.astype(jnp.float32))
        start = start + width
    query_rows = unpacked[0] * KEY_DIM ** (-0.5)
    key_rows = unpacked[1]
    decay_rows = unpacked[2]
    value_rows = unpacked[3]
    gate_rows = unpacked[4]
    retain = jnp.exp(jax.nn.log_sigmoid(decay_rows + decay_bias) / TAU)
    new_states = retain[..., None] * states + key_rows[..., :, None] * value_rows[..., None, :]
    readout = jnp.einsum("shk,shkv->shv", query_rows, new_states, precision=lax.Precision.HIGHEST)
    readout = (
        readout
        * lax.rsqrt(jnp.mean(readout * readout, axis=-1, keepdims=True) + RMS_EPS)
        * head_gain
    )
    attended = (readout * jax.nn.silu(gate_rows)).astype(jnp.bfloat16)
    seq_count, local_heads, value_width = attended.shape
    flat_width = local_heads * value_width
    collected = lax.all_gather(
        attended.reshape(1, seq_count, flat_width), ("kv", "tp"), axis=0, tiled=True
    )
    halves = lax.axis_size("tp")
    collected = collected.reshape(-1, halves, seq_count, flat_width)
    columns = out_weight.shape[1]
    out_parts = out_weight.reshape(halves, flat_width, columns)
    mixed_heads = jnp.einsum(
        "atsc,tcd->asd", collected, out_parts, preferred_element_type=jnp.float32
    ).reshape(-1, columns)
    residual_one = ALPHA * tokens.astype(jnp.float32) + mixed_heads
    offset = lax.axis_index(("kv", "tp")) * columns
    totals = lax.psum(
        (
            jnp.sum(residual_one, axis=-1, keepdims=True),
            jnp.sum(residual_one * residual_one, axis=-1, keepdims=True),
        ),
        ("kv", "tp"),
    )
    average = totals[0] / D
    spread = totals[1] / D - average * average
    normed_own = normalize(residual_one, average, spread, norm1_gain, norm1_bias)
    normed = lax.all_gather(normed_own, ("kv", "tp"), axis=1, tiled=True)
    lifted = jnp.dot(normed, up_weight, preferred_element_type=jnp.float32)
    hidden = jnp.square(jax.nn.relu(lifted)).astype(jnp.bfloat16)
    mixer_term = jnp.dot(hidden, down_weight, preferred_element_type=jnp.float32)
    mixer_all = lax.psum(mixer_term, ("kv", "tp"))
    residual_two = ALPHA * normed.astype(jnp.float32) + mixer_all
    average = jnp.sum(residual_two, axis=-1, keepdims=True) / D
    spread = jnp.sum(residual_two * residual_two, axis=-1, keepdims=True) / D - average * average
    own_rows = lax.dynamic_slice_in_dim(residual_two, offset, columns, 1)
    layer_out = normalize(own_rows, average, spread, norm2_gain, norm2_bias)
    return (layer_out, new_states)


MESH = pl.DeviceIdType.MESH
F32 = jnp.float32
BF16 = jnp.bfloat16


def dot_nt(left, right):
    return lax.dot_general(left, right, (((1,), (1,)), ((), ())), preferred_element_type=F32)


def nearest(place, count, step):
    below, above = place, count - 1 - place
    pairs = jnp.minimum(below, above)
    away = (step + 1) // 2 * (1 if step % 2 else -1)
    zigzag = jnp.where(below <= above, place - away, place + away)
    onward = jnp.where(below < above, place + (step - pairs), place - (step - pairs))
    return jnp.where(step <= 2 * pairs, zigzag, onward)


def layer_kernel(
    groups, halves, tokens, wq, wk, wd, wv, wg, bias, states, head_gain, wout, gain1, shift1,
    wup, wdown, gain2, shift2,
    out, states_out,
    proj_v, out_v, up_v, down_v, state_v, bias_v, hgain_v, gain1_v, shift1_v, gain2_v, shift2_v,
    bias_rows, x_v, acc_v, a_send, a_recv, a_rows, att_send, att_recv, x_rows, mixed_v, const_v, u_v, moments_v, both_v,
    p_send, p_recv, finals_v,
    load_sem, proj_sem, up_sem, down_sem, ready, own_ss, x_rs, a_ss, a_rs, c_ss, c_rs, t_ss, t_rs,
    u_ss, u_rs, m_ss, m_rs, p_ss, p_rs, f_ss, f_rs,
):
    my_kv, my_tp = lax.axis_index("kv"), lax.axis_index("tp")
    me = my_kv * halves + my_tp
    members, rows, cols = x_v.shape
    width = members * cols
    span = halves * cols
    seqs = rows // groups
    heads, kdim = bias_v.shape
    vdim = hgain_v.shape[1]
    kc, vc = kdim // groups, vdim // groups
    nk, nv = heads * kc, heads * vc
    top = groups - 1
    chips = [nearest(my_kv, groups, step) for step in range(groups)]
    cores = [lax.rem(my_tp + o, halves) for o in range(halves)]

    def load(src, dst, sem):
        copy = pltpu.make_async_copy(src, dst, sem)
        copy.start()
        return copy

    def chunk(chip):
        return pl.ds(pl.multiple_of(chip * span, span), span)

    loads = {}
    for index, (name, src, dst) in enumerate((
        ("tok", tokens, x_v.at[me]), ("g1", gain1, gain1_v), ("s1", shift1, shift1_v), ("bias", bias, bias_v),
    )):
        loads[name] = load(src, dst, load_sem.at[index])

    proj_loads = []

    def load_projections(step, chip):
        start = 0
        for index, weight in enumerate((wq, wk, wd, wv, wg)):
            size = weight.shape[0]
            proj_loads.append(load(
                weight.at[:, chunk(chip)], proj_v.at[pl.ds(start, size), chunk(chip)], proj_sem.at[step, index]
            ))
            start += size

    load_projections(0, chips[0])
    barrier = pltpu.get_barrier_semaphore()

    def greet(kv, tp):
        pl.semaphore_signal(barrier, inc=1, device_id={"kv": kv, "tp": tp}, device_id_type=MESH)

    @pl.when(my_kv > 0)
    def _():
        for core in cores:
            greet(my_kv - 1, core)

    for core in cores[1:]:
        greet(my_kv, core)
    for d in range(1, groups):

        @pl.when(my_kv + d < groups)
        def _():
            for core in cores:
                greet(my_kv + d, core)

    def remote(src, dst, send, recv, kv, tp):
        return pltpu.make_async_remote_copy(
            src_ref=src, dst_ref=dst, send_sem=send, recv_sem=recv, device_id={"kv": kv, "tp": tp},
            device_id_type=MESH,
        )

    def own_copy(kv, core, slot):
        return remote(x_v.at[me], x_v.at[me], own_ss.at[slot], x_rs.at[me], kv, core)

    def own_sends(first):
        plans = []
        if first:
            for o, core in enumerate(cores):
                plans.append((my_kv < top, my_kv + 1, core, o))
            for d in range(top, 0, -1):
                for o, core in enumerate(cores):
                    plans.append((my_kv >= d, my_kv - d, core, (d + 1) * halves + o))
            for o, core in enumerate(cores[1:]):
                plans.append((None, my_kv, core, halves + o))
        else:
            for d in range(2, groups):
                for o, core in enumerate(cores):
                    plans.append((my_kv + d < groups, my_kv + d, core, (groups + d - 1) * halves + o))
        return plans

    def each_own(first, act):
        for condition, kv, core, slot in own_sends(first):
            if condition is None:
                act(own_copy(kv, core, slot))
            else:

                @pl.when(condition)
                def _():
                    act(own_copy(kv, core, slot))

    def send_far():
        for d in range(2, groups):

            @pl.when(my_kv + d < groups)
            def _():
                pl.semaphore_wait(ready.at[d], halves)
                for o, core in enumerate(cores):
                    own_copy(my_kv + d, core, (groups + d - 1) * halves + o).start()

    expected = (halves - 1) + halves * my_kv + jnp.where(my_kv < top, halves, 0)
    pl.semaphore_wait(barrier, expected)
    for d in range(2, groups):

        @pl.when(my_kv >= d)
        def _():
            for core in cores:
                pl.semaphore_signal(
                    ready.at[d], inc=1, device_id={"kv": my_kv - d, "tp": core}, device_id_type=MESH
                )

    loads["tok"].wait()
    each_own(True, lambda copy: copy.start())
    load_projections(1, chips[1])
    pending = []

    def everyone():
        targets = [(chip, core) for chip in reversed(chips[1:]) for core in cores]
        return targets + [(my_kv, core) for core in cores[1:]]

    def spread(buffer, send, recv):
        for o, (chip, core) in enumerate(everyone()):
            copy = remote(buffer.at[me], buffer.at[me], send.at[o], recv.at[me], chip, core)
            copy.start()
            pending.append(copy)

    def collect(buffer, recv, chip, core):
        block = chip * halves + core
        remote(buffer.at[block], buffer.at[block], recv.at[block], recv.at[block], my_kv, my_tp).wait_recv()

    late = []
    for step, chip in enumerate(chips):
        for core in cores if step else cores[1:]:
            collect(x_v, x_rs, chip, core)
        for index in range(5):
            proj_loads[step * 5 + index].wait()
        if step + 2 < groups:
            load_projections(step + 2, chips[step + 2])
        if step == max(groups - 2, 0):
            for index, (name, src, dst) in enumerate((
                ("hg", head_gain, hgain_v), ("g2", gain2, gain2_v), ("s2", shift2, shift2_v),
                ("st", states, state_v), ("out", wout, out_v),
            )):
                loads[name] = load(src, dst, load_sem.at[4 + index])
        if step == groups - 1:
            for index, to in enumerate(chips):
                late.append(load(wup.at[chunk(to), :], up_v.at[chunk(to), :], up_sem.at[index]))
        blocks = x_v[pl.ds(chip * halves, halves)]
        left = jnp.concatenate([blocks[o] for o in range(halves)], axis=1)
        term = dot_nt(left, proj_v[:, chunk(chip)])
        acc_v[...] = acc_v[...] + term if step else term
        if step == 0:
            send_far()
            loads["g1"].wait()
            loads["s1"].wait()
            loads["bias"].wait()
            whole_shift = shift1_v[...]
            coarse = whole_shift.astype(BF16).astype(F32)
            place = lax.broadcasted_iota(jnp.int32, (rows, cols), 0)
            consts = jnp.where(place == my_tp, gain1_v[...], 0.0)
            consts = jnp.where(place == halves, coarse, consts)
            consts = jnp.where(place == halves + 1, whole_shift - coarse, consts)
            const_v[me] = consts.astype(BF16)
            for h in range(heads):
                for b in range(groups):
                    piece = jnp.broadcast_to(bias_v[h : h + 1, b * kc : (b + 1) * kc], (seqs, kc))
                    bias_rows[b * seqs : (b + 1) * seqs, h * kc : (h + 1) * kc] = piece
        if step == groups - 2:
            spread(const_v, c_ss, c_rs)
    quarter = down_v.shape[0] // 4
    down_loads = [
        load(wdown.at[pl.ds(i * quarter, quarter)], down_v.at[pl.ds(i * quarter, quarter)], down_sem.at[i])
        for i in range(4)
    ]

    for a in range(groups):
        a_send[a] = acc_v[a * seqs : (a + 1) * seqs, :].astype(BF16)
    for o, peer in enumerate(reversed(chips[1:])):
        copy = remote(a_send.at[peer], a_recv.at[my_kv], a_ss.at[o], a_rs.at[my_kv], peer, my_tp)
        copy.start()
        pending.append(copy)
    a_recv[my_kv] = a_send[my_kv]
    loads["st"].wait()
    loads["hg"].wait()
    for peer in chips[1:]:
        remote(a_send.at[peer], a_recv.at[peer], a_ss.at[0], a_rs.at[peer], my_kv, my_tp).wait_recv()
    for b in range(groups):
        a_rows[b * seqs : (b + 1) * seqs, :] = a_recv[b].astype(F32)

    q = a_rows[:, 0:nk] * KEY_DIM ** (-0.5)
    k = a_rows[:, nk : 2 * nk]
    z = a_rows[:, 2 * nk : 3 * nk] + bias_rows[...]
    retain = jnp.exp((jnp.minimum(z, 0.0) - jnp.log1p(jnp.exp(-jnp.abs(z)))) / TAU)
    product = q * k
    met = product
    for b in range(1, groups):
        met = met + pltpu.roll(product, b * seqs, 0)
    turned = jnp.concatenate([q * retain, met], axis=1).T

    def wide(s, h, first):
        start = first + h * vc
        parts = [a_rows[b * seqs + s : b * seqs + s + 1, start : start + vc] for b in range(groups)]
        return jnp.concatenate(parts, axis=1)

    strength = jnp.concatenate(
        [jnp.sum(turned[nk + h * kc : nk + (h + 1) * kc, :], axis=0, keepdims=True) for h in range(heads)], axis=0
    )
    values = []
    for s in range(seqs):
        value = jnp.concatenate([wide(s, h, 3 * nk) for h in range(heads)], axis=0)
        gate = jnp.concatenate([wide(s, h, 3 * nk + nv) for h in range(heads)], axis=0)
        values.append(value)
        lines = []
        for h in range(heads):
            total = None
            for b in range(groups):
                lane = b * seqs + s
                term = turned[h * kc : (h + 1) * kc, lane : lane + 1] * state_v[s, h, b * kc : (b + 1) * kc, :]
                total = term if total is None else total + term
            lines.append(jnp.sum(total, axis=0, keepdims=True))
        readout = jnp.concatenate(lines, axis=0) + strength[:, s : s + 1] * value
        power = jnp.mean(readout * readout, axis=-1, keepdims=True)
        readout = readout * lax.rsqrt(power + RMS_EPS) * hgain_v[...]
        attended = readout * (gate / (1.0 + jnp.exp(-gate)))
        for h in range(heads):
            att_send[s : s + 1, h * vdim : (h + 1) * vdim] = attended[h : h + 1, :].astype(BF16)
    for o, (chip, core) in enumerate(everyone()):
        copy = remote(att_send, att_recv.at[me], t_ss.at[o], t_rs.at[me], chip, core)
        copy.start()
        pending.append(copy)
    att_recv[me] = att_send[...]

    later = jnp.concatenate([retain, k], axis=1).T
    for s in range(seqs):
        for h in range(heads):
            for b in range(groups):
                lane = b * seqs + s
                subs = slice(h * kc, (h + 1) * kc)
                keys = slice(nk + h * kc, nk + (h + 1) * kc)
                states_out[s, h, b * kc : (b + 1) * kc, :] = (
                    later[subs, lane : lane + 1] * state_v[s, h, b * kc : (b + 1) * kc, :]
                    + later[keys, lane : lane + 1] * values[s][h : h + 1, :]
                )

    half = heads * vdim

    loads["out"].wait()
    for step, chip in enumerate(chips):
        for core in cores if step else cores[1:]:
            collect(att_recv, t_rs, chip, core)
        for t in range(halves):
            x_rows[step * seqs : (step + 1) * seqs, t * half : (t + 1) * half] = att_recv[chip * halves + t].astype(F32)
    mixed = jnp.dot(x_rows[...].astype(BF16), out_v[...], preferred_element_type=F32)
    for step, chip in enumerate(chips):
        mixed_v[chip] = mixed[step * seqs : (step + 1) * seqs]
    mixed = jnp.concatenate([mixed_v[a] for a in range(groups)], axis=0)
    residual = ALPHA * x_v[me].astype(F32) + mixed

    lane = lax.broadcasted_iota(jnp.int32, (rows, 128), 1)
    line = lax.broadcasted_iota(jnp.int32, (rows, 128), 0)

    def moments(block):
        center = jnp.sum(block, axis=-1, keepdims=True) / cols
        moved = block - center
        return center, moved, jnp.sum(moved * moved, axis=-1, keepdims=True)

    def as_row(center, power):
        both = jnp.where(lane == line, center, 0.0) + jnp.where(lane == line + rows, power, 0.0)
        return jnp.sum(both, axis=0, keepdims=True)

    def as_columns(row):
        center = jnp.sum(jnp.where(lane == line, row, 0.0), axis=-1, keepdims=True)
        power = jnp.sum(jnp.where(lane == line + rows, row, 0.0), axis=-1, keepdims=True)
        return center, power

    def combine(pairs):
        average = sum(center for center, _ in pairs) / members
        powers = sum(power + cols * jnp.square(center - average) for center, power in pairs)
        return average, lax.rsqrt(powers / width + LN_EPS)

    center, moved, power = moments(residual)
    u_v[me] = (moved * gain1_v[...]).astype(BF16)
    moments_v[me] = as_row(center, power)
    spread(u_v, u_ss, u_rs)
    spread(moments_v, m_ss, m_rs)

    for step, chip in enumerate(chips):
        for core in cores if step else cores[1:]:
            collect(const_v, c_rs, chip, core)
    lifted = fixed = None
    pairs = []
    for step, chip in enumerate(chips):
        late[step].wait()
        for core in cores if step else cores[1:]:
            collect(u_v, u_rs, chip, core)
            collect(moments_v, m_rs, chip, core)
        left = []
        for o in range(halves):
            block = chip * halves + o
            left.append(jnp.concatenate([u_v[block], const_v[block]], axis=0))
            pairs.append(as_columns(moments_v[block]))
        term = jnp.dot(jnp.concatenate(left, axis=1), up_v[chunk(chip), :], preferred_element_type=F32)
        main, extra = term[:rows], term[rows:]
        for o in range(halves):
            main = main + pairs[step * halves + o][0] * extra[o : o + 1]
        lifted = main if lifted is None else lifted + main
        fixed = extra if fixed is None else fixed + extra
    average, scale = combine(pairs)
    slope = sum(fixed[o : o + 1] for o in range(halves))
    lifted = scale * (lifted - average * slope) + (fixed[halves : halves + 1] + fixed[halves + 1 : halves + 2])
    hidden = jnp.square(jnp.maximum(lifted, 0.0)).astype(BF16)
    normed = ((residual - average) * scale * gain1_v[...] + shift1_v[...]).astype(BF16)

    def block_of(chip, core):
        return pl.ds(pl.multiple_of((chip * halves + core) * cols, cols), cols)

    for copy in down_loads:
        copy.wait()
    for step in range(top, -1, -1):
        chip = chips[step]
        both = jnp.dot(hidden, down_v[:, chunk(chip)], preferred_element_type=F32)
        if step:
            for core in range(halves):
                o = (top - step) * halves + core
                p_send[o] = both[:, core * cols : (core + 1) * cols].astype(BF16)
                copy = remote(p_send.at[o], p_recv.at[me], p_ss.at[o], p_rs.at[me], chip, core)
                copy.start()
                pending.append(copy)
        else:
            both_v[...] = both
    for o, core in enumerate(cores[1:]):
        p_send[top * halves + o] = both_v[:, block_of(0, core)].astype(BF16)
        copy = remote(
            p_send.at[top * halves + o], p_recv.at[me], p_ss.at[top * halves + o], p_rs.at[me], my_kv, core
        )
        copy.start()
        pending.append(copy)
    total = both_v[:, block_of(0, my_tp)]
    total = total + ALPHA * normed.astype(F32)
    for chip, core in everyone():
        collect(p_recv, p_rs, chip, core)
        total = total + p_recv[chip * halves + core].astype(F32)
    center, moved, power = moments(total)
    finals_v[me] = as_row(center, power)
    spread(finals_v, f_ss, f_rs)
    pairs = [(center, power)]
    loads["g2"].wait()
    loads["s2"].wait()
    for chip, core in reversed(everyone()):
        collect(finals_v, f_rs, chip, core)
        pairs.append(as_columns(finals_v[chip * halves + core]))
    average, scale = combine(pairs)
    out[...] = ((total - average) * scale * gain2_v[...] + shift2_v[...]).astype(BF16)

    each_own(True, lambda copy: copy.wait_send())
    each_own(False, lambda copy: copy.wait_send())
    for copy in pending:
        copy.wait_send()


def finish_kernel(result, fresh, out, states_out, sems):
    puts = [
        pltpu.make_async_copy(fresh, states_out, sems.at[0]),
        pltpu.make_async_copy(result, out, sems.at[1]),
    ]
    for put in puts:
        put.start()
    for put in puts:
        put.wait()


def fused(groups, halves, *arrays):
    (tokens, wq, wk, wv, wg, wd, bias, states, head_gain, wout, gain1, shift1, wup, wdown, gain2,
     shift2) = arrays

    def flat(weight):
        return weight.transpose(1, 2, 0).reshape(-1, weight.shape[0])

    def row(vector):
        return vector.reshape(1, -1)

    rows, cols = tokens.shape
    members = groups * halves
    width = wq.shape[0]
    seqs, heads, kdim, vdim = states.shape
    proj = 3 * wq.shape[1] * wq.shape[2] + 2 * wv.shape[1] * wv.shape[2]
    vmem = pltpu.VMEM
    dma = pltpu.SemaphoreType.DMA
    anywhere = pl.BlockSpec(memory_space=pl.ANY)
    inside = pl.BlockSpec(memory_space=pltpu.VMEM)
    scratch = [
        vmem((proj, width), BF16),
        vmem(wout.shape, BF16),
        vmem(wup.shape, BF16),
        vmem(wdown.shape, BF16),
        vmem(states.shape, F32),
        vmem(bias.shape, F32),
        vmem(head_gain.shape, F32),
        vmem((1, cols), F32),
        vmem((1, cols), F32),
        vmem((1, cols), F32),
        vmem((1, cols), F32),
        vmem((rows, heads * kdim // groups), F32),
        vmem((members, rows, cols), BF16),
        vmem((rows, proj), F32),
        vmem((groups, seqs, proj), BF16),
        vmem((groups, seqs, proj), BF16),
        vmem((rows, proj), F32),
        vmem((seqs, heads * vdim), BF16),
        vmem((members, seqs, heads * vdim), BF16),
        vmem((rows, halves * heads * vdim), F32),
        vmem((groups, seqs, cols), F32),
        vmem((members, rows, cols), BF16),
        vmem((members, rows, cols), BF16),
        vmem((members, 1, 128), F32),
        vmem((rows, halves * cols), F32),
        vmem((members - 1, rows, cols), BF16),
        vmem((members, rows, cols), BF16),
        vmem((members, 1, 128), F32),
        dma((9,)),
        dma((groups, 5)),
        dma((groups,)),
        dma((4,)),
        pltpu.SemaphoreType.REGULAR((groups,)),
        dma((2 * groups * halves,)),
        dma((members,)),
        dma((groups,)),
        dma((groups,)),
    ]
    scratch += [dma((members,))] * 12
    result, fresh = pl.pallas_call(
        functools.partial(layer_kernel, groups, halves),
        out_shape=(
            vmem(tokens.shape, BF16),
            vmem(states.shape, F32),
        ),
        in_specs=[anywhere] * 16,
        out_specs=(inside, inside),
        scratch_shapes=scratch,
        compiler_params=pltpu.CompilerParams(
            collective_id=0, has_side_effects=True, vmem_limit_bytes=58*1024*1024
        ),
    )(
        tokens, flat(wq), flat(wk), flat(wd), flat(wv), flat(wg), bias, states, head_gain, wout,
        row(gain1), row(shift1), wup, wdown, row(gain2), row(shift2),
    )
    return pl.pallas_call(
        finish_kernel,
        out_shape=(
            jax.ShapeDtypeStruct(tokens.shape, BF16),
            jax.ShapeDtypeStruct(states.shape, F32),
        ),
        in_specs=[anywhere] * 2,
        out_specs=(anywhere, anywhere),
        scratch_shapes=[dma((2,))],
        compiler_params=pltpu.CompilerParams(vmem_limit_bytes=1048576),
    )(result, fresh)


def dispatch(groups, halves, *arrays):
    rows, cols = arrays[0].shape
    if rows == 8 and cols % 128 == 0 and rows % groups == 0 and groups > 2 and halves <= 4:
        return fused(groups, halves, *arrays)
    return body(*arrays)


def solution(mesh):
    placed = (
        P("dp", ("kv", "tp")),
        P(None, "tp", "kv"),
        P(None, "tp", "kv"),
        P(None, "tp", "kv"),
        P(None, "tp", "kv"),
        P(None, "tp", "kv"),
        P("tp", None),
        P(("dp", "kv"), "tp", None, None),
        P("tp", None),
        P(None, ("kv", "tp")),
        P(("kv", "tp")),
        P(("kv", "tp")),
        P(None, ("kv", "tp")),
        P(("kv", "tp"), None),
        P(("kv", "tp")),
        P(("kv", "tp")),
    )
    return jax.shard_map(
        functools.partial(dispatch, mesh.shape["kv"], mesh.shape["tp"]),
        mesh=mesh,
        in_specs=placed,
        out_specs=(P("dp", ("kv", "tp")), P(("dp", "kv"), "tp", None, None)),
        check_vma=False,
    )
```

```python
import functools

import jax
import jax.numpy as jnp
from jax import lax
from jax.experimental import pallas as pl
from jax.experimental.pallas import tpu as pltpu
from jax.sharding import PartitionSpec as P

D = 4096
KEY_DIM = 128


ALPHA = 2.0**0.5
TAU = 16.0
LN_EPS = 1e-05
RMS_EPS = 1e-06


def project_flat(inputs, weight):
    flattened = weight.reshape(weight.shape[0], -1)
    return jnp.dot(inputs, flattened, preferred_element_type=jnp.float32).astype(jnp.bfloat16)


def normalize(inputs, average, spread, row_gain, row_shift):
    return ((inputs - average) * lax.rsqrt(spread + LN_EPS) * row_gain + row_shift).astype(
        jnp.bfloat16
    )


def body(
    tokens,
    query_weight,
    key_weight,
    value_weight,
    gate_weight,
    decay_weight,
    decay_bias,
    states,
    head_gain,
    out_weight,
    norm1_gain,
    norm1_bias,
    up_weight,
    down_weight,
    norm2_gain,
    norm2_bias,
):
    whole = lax.all_gather(tokens, ("kv", "tp"), axis=1, tiled=True)
    weights_list = (query_weight, key_weight, decay_weight, value_weight, gate_weight)
    packed = jnp.concatenate([project_flat(whole, weight) for weight in weights_list], axis=1)
    arrived = lax.all_to_all(packed, "kv", split_axis=0, concat_axis=0, tiled=True)
    groups = lax.axis_size("kv")
    seq_count = whole.shape[0] // groups
    local_heads = query_weight.shape[1]
    unpacked = []
    start = 0
    for weight in weights_list:
        channels = weight.shape[2]
        width = local_heads * channels
        block = arrived[:, start : start + width].reshape(groups, seq_count, local_heads, channels)
        block = block.transpose(1, 2, 0, 3).reshape(seq_count, local_heads, groups * channels)
        unpacked.append(block.astype(jnp.float32))
        start = start + width
    query_rows = unpacked[0] * KEY_DIM ** (-0.5)
    key_rows = unpacked[1]
    decay_rows = unpacked[2]
    value_rows = unpacked[3]
    gate_rows = unpacked[4]
    retain = jnp.exp(jax.nn.log_sigmoid(decay_rows + decay_bias) / TAU)
    new_states = retain[..., None] * states + key_rows[..., :, None] * value_rows[..., None, :]
    readout = jnp.einsum("shk,shkv->shv", query_rows, new_states, precision=lax.Precision.HIGHEST)
    readout = (
        readout
        * lax.rsqrt(jnp.mean(readout * readout, axis=-1, keepdims=True) + RMS_EPS)
        * head_gain
    )
    attended = (readout * jax.nn.silu(gate_rows)).astype(jnp.bfloat16)
    seq_count, local_heads, value_width = attended.shape
    flat_width = local_heads * value_width
    collected = lax.all_gather(
        attended.reshape(1, seq_count, flat_width), ("kv", "tp"), axis=0, tiled=True
    )
    halves = lax.axis_size("tp")
    collected = collected.reshape(-1, halves, seq_count, flat_width)
    columns = out_weight.shape[1]
    out_parts = out_weight.reshape(halves, flat_width, columns)
    mixed_heads = jnp.einsum(
        "atsc,tcd->asd", collected, out_parts, preferred_element_type=jnp.float32
    ).reshape(-1, columns)
    residual_one = ALPHA * tokens.astype(jnp.float32) + mixed_heads
    offset = lax.axis_index(("kv", "tp")) * columns
    totals = lax.psum(
        (
            jnp.sum(residual_one, axis=-1, keepdims=True),
            jnp.sum(residual_one * residual_one, axis=-1, keepdims=True),
        ),
        ("kv", "tp"),
    )
    average = totals[0] / D
    spread = totals[1] / D - average * average
    normed_own = normalize(residual_one, average, spread, norm1_gain, norm1_bias)
    normed = lax.all_gather(normed_own, ("kv", "tp"), axis=1, tiled=True)
    lifted = jnp.dot(normed, up_weight, preferred_element_type=jnp.float32)
    hidden = jnp.square(jax.nn.relu(lifted)).astype(jnp.bfloat16)
    mixer_term = jnp.dot(hidden, down_weight, preferred_element_type=jnp.float32)
    mixer_all = lax.psum(mixer_term, ("kv", "tp"))
    residual_two = ALPHA * normed.astype(jnp.float32) + mixer_all
    average = jnp.sum(residual_two, axis=-1, keepdims=True) / D
    spread = jnp.sum(residual_two * residual_two, axis=-1, keepdims=True) / D - average * average
    own_rows = lax.dynamic_slice_in_dim(residual_two, offset, columns, 1)
    layer_out = normalize(own_rows, average, spread, norm2_gain, norm2_bias)
    return (layer_out, new_states)


MESH = pl.DeviceIdType.MESH
F32 = jnp.float32
BF16 = jnp.bfloat16


def dot_nt(left, right):
    return lax.dot_general(left, right, (((1,), (1,)), ((), ())), preferred_element_type=F32)


def nearest(place, count, step, lower):
    below, above = place, count - 1 - place
    pairs = jnp.minimum(below, above)
    away = (step + 1) // 2 * (1 if step % 2 else -1)
    zigzag = jnp.where(lower, place - away, place + away)
    onward = jnp.where(below < above, place + (step - pairs), place - (step - pairs))
    return jnp.where(step <= 2 * pairs, zigzag, onward)


def layer_kernel(
    groups, halves, tokens, wq, wk, wd, wv, wg, bias, states, head_gain, wout, gain1, shift1,
    wup, wdown, gain2, shift2,
    out, states_out,
    proj_v, out_v, up_v, down_v, state_v, bias_v, hgain_v, gain1_v, shift1_v, gain2_v, shift2_v,
    bias_rows, x_v, acc_v, a_send, a_recv, a_rows, att_send, att_recv, x_rows, mixed_v, const_v, u_v, moments_v, both_v,
    p_send, p_recv, finals_v,
    load_sem, proj_sem, up_sem, down_sem, ready, own_ss, x_rs, a_ss, a_rs, c_ss, c_rs, t_ss, t_rs,
    u_ss, u_rs, m_ss, m_rs, p_ss, p_rs, f_ss, f_rs,
):
    my_kv, my_tp = lax.axis_index("kv"), lax.axis_index("tp")
    me = my_kv * halves + my_tp
    members, rows, cols = x_v.shape
    width = members * cols
    span = halves * cols
    seqs = rows // groups
    heads, kdim = bias_v.shape
    vdim = hgain_v.shape[1]
    kc, vc = kdim // groups, vdim // groups
    nk, nv = heads * kc, heads * vc
    top = groups - 1
    low_half = 2 * my_kv <= top
    rising = [nearest(my_kv, groups, step, my_kv >= 0) for step in range(groups)]
    chips = [nearest(my_kv, groups, step, low_half) for step in range(groups)]
    inward = [nearest(my_kv, groups, step, jnp.logical_not(low_half)) for step in range(groups)]
    cores = [lax.rem(my_tp + o, halves) for o in range(halves)]

    def load(src, dst, sem):
        copy = pltpu.make_async_copy(src, dst, sem)
        copy.start()
        return copy

    def chunk(chip):
        return pl.ds(pl.multiple_of(chip * span, span), span)

    loads = {}
    for index, (name, src, dst) in enumerate((
        ("tok", tokens, x_v.at[me]), ("g1", gain1, gain1_v), ("s1", shift1, shift1_v), ("bias", bias, bias_v),
    )):
        loads[name] = load(src, dst, load_sem.at[index])

    proj_loads = []

    def load_projections(step, chip):
        start = 0
        for index, weight in enumerate((wq, wk, wd, wv, wg)):
            size = weight.shape[0]
            proj_loads.append(load(
                weight.at[:, chunk(chip)], proj_v.at[pl.ds(start, size), chunk(chip)], proj_sem.at[step, index]
            ))
            start += size

    load_projections(0, rising[0])
    barrier = pltpu.get_barrier_semaphore()

    def greet(kv, tp):
        pl.semaphore_signal(barrier, inc=1, device_id={"kv": kv, "tp": tp}, device_id_type=MESH)

    @pl.when(my_kv > 0)
    def _():
        for core in cores:
            greet(my_kv - 1, core)

    for core in cores[1:]:
        greet(my_kv, core)
    for d in range(2, groups):

        @pl.when(my_kv + d < groups)
        def _():
            for core in cores:
                greet(my_kv + d, core)

    def remote(src, dst, send, recv, kv, tp):
        return pltpu.make_async_remote_copy(
            src_ref=src, dst_ref=dst, send_sem=send, recv_sem=recv, device_id={"kv": kv, "tp": tp},
            device_id_type=MESH,
        )

    def own_copy(kv, core, slot):
        return remote(x_v.at[me], x_v.at[me], own_ss.at[slot], x_rs.at[me], kv, core)

    def own_sends(first):
        plans = []
        if first:
            for o, core in enumerate(cores):
                plans.append((my_kv < top, my_kv + 1, core, o))
            for d in range(top, 1, -1):
                for o, core in enumerate(cores):
                    plans.append((my_kv >= d, my_kv - d, core, (d + 1) * halves + o))
            for o, core in enumerate(cores[1:]):
                plans.append((None, my_kv, core, halves + o))
        else:
            for o, core in enumerate(cores):
                plans.append((my_kv > 0, my_kv - 1, core, 2 * halves + o))
            for d in range(2, groups):
                for o, core in enumerate(cores):
                    plans.append((my_kv + d < groups, my_kv + d, core, (groups + d - 1) * halves + o))
        return plans

    def each_own(first, act):
        for condition, kv, core, slot in own_sends(first):
            if condition is None:
                act(own_copy(kv, core, slot))
            else:

                @pl.when(condition)
                def _():
                    act(own_copy(kv, core, slot))

    def send_below():
        pl.semaphore_wait(ready.at[1], halves)
        for o, core in enumerate(cores):
            own_copy(my_kv - 1, core, 2 * halves + o).start()

    def send_far():
        for d in range(top, 1, -1):

            @pl.when(my_kv + d < groups)
            def _():
                pl.semaphore_wait(ready.at[d], halves)
                for o, core in enumerate(cores):
                    own_copy(my_kv + d, core, (groups + d - 1) * halves + o).start()

    expected = (halves - 1) + halves * jnp.maximum(my_kv - 1, 0) + jnp.where(my_kv < top, halves, 0)
    pl.semaphore_wait(barrier, expected)
    for d in range(2, groups):

        @pl.when(my_kv >= d)
        def _():
            for core in cores:
                pl.semaphore_signal(
                    ready.at[d], inc=1, device_id={"kv": my_kv - d, "tp": core}, device_id_type=MESH
                )

    @pl.when(my_kv < top)
    def _():
        for core in cores:
            pl.semaphore_signal(
                ready.at[1], inc=1, device_id={"kv": my_kv + 1, "tp": core}, device_id_type=MESH
            )

    loads["tok"].wait()
    each_own(True, lambda copy: copy.start())
    load_projections(1, rising[1])
    pending = []

    def everyone():
        targets = [(chip, core) for chip in reversed(chips[1:]) for core in range(halves)]
        return targets + [(my_kv, core) for core in cores[1:]]

    def spread(buffer, send, recv):
        for o, (chip, core) in enumerate(everyone()):
            copy = remote(buffer.at[me], buffer.at[me], send.at[o], recv.at[me], chip, core)
            copy.start()
            pending.append(copy)

    def collect(buffer, recv, chip, core):
        block = chip * halves + core
        remote(buffer.at[block], buffer.at[block], recv.at[block], recv.at[block], my_kv, my_tp).wait_recv()

    late = []
    for step, chip in enumerate(rising):
        for core in cores if step else cores[1:]:
            collect(x_v, x_rs, chip, core)
        for index in range(5):
            proj_loads[step * 5 + index].wait()
        if step + 2 < groups:
            load_projections(step + 2, rising[step + 2])
        if step == max(groups - 2, 0):
            for index, (name, src, dst) in enumerate((
                ("hg", head_gain, hgain_v), ("g2", gain2, gain2_v), ("s2", shift2, shift2_v),
                ("st", states, state_v), ("out", wout, out_v),
            )):
                loads[name] = load(src, dst, load_sem.at[4 + index])
        if step == groups - 1:
            for index, to in enumerate(inward):
                late.append(load(wup.at[chunk(to), :], up_v.at[chunk(to), :], up_sem.at[index]))

        if step == 0:

            @pl.when(my_kv > 0)
            def _():
                send_below()
                send_far()

        @pl.when(my_kv >= 0)
        def _():
            blocks = x_v[pl.ds(chip * halves, halves)]
            left = jnp.concatenate([blocks[o] for o in range(halves)], axis=1)
            term = dot_nt(left, proj_v[:, chunk(chip)])
            acc_v[...] = acc_v[...] + term if step else term

        if step == 0:

            @pl.when(my_kv == 0)
            def _():
                send_far()

            loads["g1"].wait()
            loads["s1"].wait()
            loads["bias"].wait()
            whole_shift = shift1_v[...]
            coarse = whole_shift.astype(BF16).astype(F32)
            place = lax.broadcasted_iota(jnp.int32, (rows, cols), 0)
            consts = jnp.where(place == my_tp, gain1_v[...], 0.0)
            consts = jnp.where(place == halves, coarse, consts)
            consts = jnp.where(place == halves + 1, whole_shift - coarse, consts)
            const_v[me] = consts.astype(BF16)
            for h in range(heads):
                for b in range(groups):
                    piece = jnp.broadcast_to(bias_v[h : h + 1, b * kc : (b + 1) * kc], (seqs, kc))
                    bias_rows[b * seqs : (b + 1) * seqs, h * kc : (h + 1) * kc] = piece
        if step == groups - 2:
            spread(const_v, c_ss, c_rs)
    quarter = down_v.shape[0] // 4
    down_loads = [
        load(wdown.at[pl.ds(i * quarter, quarter)], down_v.at[pl.ds(i * quarter, quarter)], down_sem.at[i])
        for i in range(4)
    ]

    for a in range(groups):
        a_send[a] = acc_v[a * seqs : (a + 1) * seqs, :].astype(BF16)
    for o, peer in enumerate(reversed(chips[1:])):
        copy = remote(a_send.at[peer], a_recv.at[my_kv], a_ss.at[o], a_rs.at[my_kv], peer, my_tp)
        copy.start()
        pending.append(copy)
    a_recv[my_kv] = a_send[my_kv]
    loads["st"].wait()
    loads["hg"].wait()
    for peer in chips[1:]:
        remote(a_send.at[peer], a_recv.at[peer], a_ss.at[0], a_rs.at[peer], my_kv, my_tp).wait_recv()
    for b in range(groups):
        a_rows[b * seqs : (b + 1) * seqs, :] = a_recv[b].astype(F32)

    q = a_rows[:, 0:nk] * KEY_DIM ** (-0.5)
    k = a_rows[:, nk : 2 * nk]
    z = a_rows[:, 2 * nk : 3 * nk] + bias_rows[...]
    retain = jnp.exp((jnp.minimum(z, 0.0) - jnp.log1p(jnp.exp(-jnp.abs(z)))) / TAU)
    product = q * k
    met = product
    for b in range(1, groups):
        met = met + pltpu.roll(product, b * seqs, 0)
    turned = jnp.concatenate([q * retain, met], axis=1).T

    def wide(s, h, first):
        start = first + h * vc
        parts = [a_rows[b * seqs + s : b * seqs + s + 1, start : start + vc] for b in range(groups)]
        return jnp.concatenate(parts, axis=1)

    strength = jnp.concatenate(
        [jnp.sum(turned[nk + h * kc : nk + (h + 1) * kc, :], axis=0, keepdims=True) for h in range(heads)], axis=0
    )
    values = []
    for s in range(seqs):
        value = jnp.concatenate([wide(s, h, 3 * nk) for h in range(heads)], axis=0)
        gate = jnp.concatenate([wide(s, h, 3 * nk + nv) for h in range(heads)], axis=0)
        values.append(value)
        totals = [None] * heads
        for b in range(groups):
            lane = b * seqs + s
            column = jnp.broadcast_to(turned[0:nk, lane : lane + 1], (nk, 128))
            for h in range(heads):
                for low in range(0, kc, 8):
                    block = state_v[s, h, b * kc + low : b * kc + low + 8, :]
                    part = column[h * kc + low : h * kc + low + 8]
                    term = jnp.concatenate([part] * (vdim // 128), axis=1) * block
                    totals[h] = term if totals[h] is None else totals[h] + term
        lines = [jnp.sum(total, axis=0, keepdims=True) for total in totals]
        readout = jnp.concatenate(lines, axis=0) + strength[:, s : s + 1] * value
        power = jnp.mean(readout * readout, axis=-1, keepdims=True)
        readout = readout * lax.rsqrt(power + RMS_EPS) * hgain_v[...]
        attended = readout * (gate / (1.0 + jnp.exp(-gate)))
        for h in range(heads):
            att_send[s : s + 1, h * vdim : (h + 1) * vdim] = attended[h : h + 1, :].astype(BF16)
    for o, (chip, core) in enumerate(everyone()):
        copy = remote(att_send, att_recv.at[me], t_ss.at[o], t_rs.at[me], chip, core)
        copy.start()
        pending.append(copy)
    att_recv[me] = att_send[...]

    later = jnp.concatenate([retain, k], axis=1).T
    for s in range(seqs):
        for h in range(heads):
            for b in range(groups):
                lane = b * seqs + s
                subs = slice(h * kc, (h + 1) * kc)
                keys = slice(nk + h * kc, nk + (h + 1) * kc)
                states_out[s, h, b * kc : (b + 1) * kc, :] = (
                    later[subs, lane : lane + 1] * state_v[s, h, b * kc : (b + 1) * kc, :]
                    + later[keys, lane : lane + 1] * values[s][h : h + 1, :]
                )

    half = heads * vdim

    loads["out"].wait()
    for step, chip in enumerate(chips):
        for core in cores if step else cores[1:]:
            collect(att_recv, t_rs, chip, core)
        for t in range(halves):
            x_rows[step * seqs : (step + 1) * seqs, t * half : (t + 1) * half] = att_recv[chip * halves + t]

    @pl.when(my_kv >= 0)
    def _():
        mixed = jnp.dot(x_rows[...], out_v[...], preferred_element_type=F32)
        for step, chip in enumerate(chips):
            mixed_v[chip] = mixed[step * seqs : (step + 1) * seqs]

    mixed = jnp.concatenate([mixed_v[a] for a in range(groups)], axis=0)
    residual = ALPHA * x_v[me].astype(F32) + mixed

    lane = lax.broadcasted_iota(jnp.int32, (rows, 128), 1)
    line = lax.broadcasted_iota(jnp.int32, (rows, 128), 0)

    def moments(block):
        center = jnp.sum(block, axis=-1, keepdims=True) / cols
        moved = block - center
        return center, moved, jnp.sum(moved * moved, axis=-1, keepdims=True)

    def as_row(center, power):
        both = jnp.where(lane == line, center, 0.0) + jnp.where(lane == line + rows, power, 0.0)
        return jnp.sum(both, axis=0, keepdims=True)

    def as_columns(row):
        center = jnp.sum(jnp.where(lane == line, row, 0.0), axis=-1, keepdims=True)
        power = jnp.sum(jnp.where(lane == line + rows, row, 0.0), axis=-1, keepdims=True)
        return center, power

    def combine(pairs):
        average = sum(center for center, _ in pairs) / members
        powers = sum(power + cols * jnp.square(center - average) for center, power in pairs)
        return average, lax.rsqrt(powers / width + LN_EPS)

    center, moved, power = moments(residual)
    u_v[me] = (moved * gain1_v[...]).astype(BF16)
    moments_v[me] = as_row(center, power)
    spread(moments_v, m_ss, m_rs)
    spread(u_v, u_ss, u_rs)

    for step, chip in enumerate(chips):
        for core in cores if step else cores[1:]:
            collect(const_v, c_rs, chip, core)
    lifted = fixed = None
    pairs = []
    for step, chip in enumerate(inward):
        late[step].wait()
        for core in cores if step else cores[1:]:
            collect(u_v, u_rs, chip, core)
            collect(moments_v, m_rs, chip, core)
        left = []
        for o in range(halves):
            block = chip * halves + o
            left.append(jnp.concatenate([u_v[block], const_v[block]], axis=0))
            pairs.append(as_columns(moments_v[block]))
        term = jnp.dot(jnp.concatenate(left, axis=1), up_v[chunk(chip), :], preferred_element_type=F32)
        main, extra = term[:rows], term[rows:]
        for o in range(halves):
            main = main + pairs[step * halves + o][0] * extra[o : o + 1]
        lifted = main if lifted is None else lifted + main
        fixed = extra if fixed is None else fixed + extra
    average, scale = combine(pairs)
    slope = sum(fixed[o : o + 1] for o in range(halves))
    lifted = scale * (lifted - average * slope) + (fixed[halves : halves + 1] + fixed[halves + 1 : halves + 2])
    hidden = jnp.square(jnp.maximum(lifted, 0.0)).astype(BF16)
    normed = ((residual - average) * scale * gain1_v[...] + shift1_v[...]).astype(BF16)

    def block_of(chip, core):
        return pl.ds(pl.multiple_of((chip * halves + core) * cols, cols), cols)

    for copy in down_loads:
        copy.wait()
    def send_sum(o, value, chip, core):
        p_send[o] = value.astype(BF16)
        copy = remote(p_send.at[o], p_recv.at[me], p_ss.at[o], p_rs.at[me], chip, core)
        copy.start()
        pending.append(copy)

    for step in range(top, 0, -1):
        both = jnp.dot(hidden, down_v[:, chunk(chips[step])], preferred_element_type=F32)
        for core in range(halves):
            send_sum((top - step) * halves + core, both[:, core * cols : (core + 1) * cols], chips[step], core)
    both_v[...] = jnp.dot(hidden, down_v[:, chunk(my_kv)], preferred_element_type=F32)
    for o, core in enumerate(cores[1:]):
        send_sum(top * halves + o, both_v[:, block_of(0, core)], my_kv, core)
    total = both_v[:, block_of(0, my_tp)]
    total = total + ALPHA * normed.astype(F32)
    for chip, core in everyone():
        collect(p_recv, p_rs, chip, core)
        total = total + p_recv[chip * halves + core].astype(F32)
    center, moved, power = moments(total)
    finals_v[me] = as_row(center, power)
    spread(finals_v, f_ss, f_rs)
    pairs = [(center, power)]
    loads["g2"].wait()
    loads["s2"].wait()
    for chip, core in reversed(everyone()):
        collect(finals_v, f_rs, chip, core)
        pairs.append(as_columns(finals_v[chip * halves + core]))
    average, scale = combine(pairs)
    out[...] = ((total - average) * scale * gain2_v[...] + shift2_v[...]).astype(BF16)

    each_own(True, lambda copy: copy.wait_send())
    each_own(False, lambda copy: copy.wait_send())
    for copy in pending:
        copy.wait_send()


def finish_kernel(result, fresh, out, states_out, sems):
    puts = [
        pltpu.make_async_copy(fresh, states_out, sems.at[0]),
        pltpu.make_async_copy(result, out, sems.at[1]),
    ]
    for put in puts:
        put.start()
    for put in puts:
        put.wait()


def fused(groups, halves, *arrays):
    (tokens, wq, wk, wv, wg, wd, bias, states, head_gain, wout, gain1, shift1, wup, wdown, gain2,
     shift2) = arrays

    def flat(weight):
        return weight.transpose(1, 2, 0).reshape(-1, weight.shape[0])

    def row(vector):
        return vector.reshape(1, -1)

    rows, cols = tokens.shape
    members = groups * halves
    width = wq.shape[0]
    seqs, heads, kdim, vdim = states.shape
    proj = 3 * wq.shape[1] * wq.shape[2] + 2 * wv.shape[1] * wv.shape[2]
    vmem = pltpu.VMEM
    dma = pltpu.SemaphoreType.DMA
    anywhere = pl.BlockSpec(memory_space=pl.ANY)
    inside = pl.BlockSpec(memory_space=pltpu.VMEM)
    scratch = [
        vmem((proj, width), BF16),
        vmem(wout.shape, BF16),
        vmem(wup.shape, BF16),
        vmem(wdown.shape, BF16),
        vmem(states.shape, F32),
        vmem(bias.shape, F32),
        vmem(head_gain.shape, F32),
        vmem((1, cols), F32),
        vmem((1, cols), F32),
        vmem((1, cols), F32),
        vmem((1, cols), F32),
        vmem((rows, heads * kdim // groups), F32),
        vmem((members, rows, cols), BF16),
        vmem((rows, proj), F32),
        vmem((groups, seqs, proj), BF16),
        vmem((groups, seqs, proj), BF16),
        vmem((rows, proj), F32),
        vmem((seqs, heads * vdim), BF16),
        vmem((members, seqs, heads * vdim), BF16),
        vmem((rows, halves * heads * vdim), BF16),
        vmem((groups, seqs, cols), F32),
        vmem((members, rows, cols), BF16),
        vmem((members, rows, cols), BF16),
        vmem((members, 1, 128), F32),
        vmem((rows, halves * cols), F32),
        vmem((members - 1, rows, cols), BF16),
        vmem((members, rows, cols), BF16),
        vmem((members, 1, 128), F32),
        dma((9,)),
        dma((groups, 5)),
        dma((groups,)),
        dma((4,)),
        pltpu.SemaphoreType.REGULAR((groups,)),
        dma((2 * groups * halves,)),
        dma((members,)),
        dma((groups,)),
        dma((groups,)),
    ]
    scratch += [dma((members,))] * 12
    result, fresh = pl.pallas_call(
        functools.partial(layer_kernel, groups, halves),
        out_shape=(
            vmem(tokens.shape, BF16),
            vmem(states.shape, F32),
        ),
        in_specs=[anywhere] * 16,
        out_specs=(inside, inside),
        scratch_shapes=scratch,
        compiler_params=pltpu.CompilerParams(
            collective_id=0, has_side_effects=True, vmem_limit_bytes=58*1024*1024
        ),
    )(
        tokens, flat(wq), flat(wk), flat(wd), flat(wv), flat(wg), bias, states, head_gain, wout,
        row(gain1), row(shift1), wup, wdown, row(gain2), row(shift2),
    )
    return pl.pallas_call(
        finish_kernel,
        out_shape=(
            jax.ShapeDtypeStruct(tokens.shape, BF16),
            jax.ShapeDtypeStruct(states.shape, F32),
        ),
        in_specs=[anywhere] * 2,
        out_specs=(anywhere, anywhere),
        scratch_shapes=[dma((2,))],
        compiler_params=pltpu.CompilerParams(vmem_limit_bytes=1048576),
    )(result, fresh)


def dispatch(groups, halves, *arrays):
    rows, cols = arrays[0].shape
    if rows == 8 and cols % 128 == 0 and rows % groups == 0 and groups > 2 and halves <= 4:
        return fused(groups, halves, *arrays)
    return body(*arrays)


def solution(mesh):
    placed = (
        P("dp", ("kv", "tp")),
        P(None, "tp", "kv"),
        P(None, "tp", "kv"),
        P(None, "tp", "kv"),
        P(None, "tp", "kv"),
        P(None, "tp", "kv"),
        P("tp", None),
        P(("dp", "kv"), "tp", None, None),
        P("tp", None),
        P(None, ("kv", "tp")),
        P(("kv", "tp")),
        P(("kv", "tp")),
        P(None, ("kv", "tp")),
        P(("kv", "tp"), None),
        P(("kv", "tp")),
        P(("kv", "tp")),
    )
    return jax.shard_map(
        functools.partial(dispatch, mesh.shape["kv"], mesh.shape["tp"]),
        mesh=mesh,
        in_specs=placed,
        out_specs=(P("dp", ("kv", "tp")), P(("dp", "kv"), "tp", None, None)),
        check_vma=False,
    )
```

```python
import functools

import jax
import jax.numpy as jnp
from jax import lax
from jax.experimental import pallas as pl
from jax.experimental.pallas import tpu as pltpu
from jax.sharding import PartitionSpec as P

D = 4096
KEY_DIM = 128


ALPHA = 2.0**0.5
TAU = 16.0
LN_EPS = 1e-05
RMS_EPS = 1e-06


def project_flat(inputs, weight):
    flattened = weight.reshape(weight.shape[0], -1)
    return jnp.dot(inputs, flattened, preferred_element_type=jnp.float32).astype(jnp.bfloat16)


def normalize(inputs, average, spread, row_gain, row_shift):
    return ((inputs - average) * lax.rsqrt(spread + LN_EPS) * row_gain + row_shift).astype(
        jnp.bfloat16
    )


def body(
    tokens,
    query_weight,
    key_weight,
    value_weight,
    gate_weight,
    decay_weight,
    decay_bias,
    states,
    head_gain,
    out_weight,
    norm1_gain,
    norm1_bias,
    up_weight,
    down_weight,
    norm2_gain,
    norm2_bias,
):
    whole = lax.all_gather(tokens, ("kv", "tp"), axis=1, tiled=True)
    weights_list = (query_weight, key_weight, decay_weight, value_weight, gate_weight)
    packed = jnp.concatenate([project_flat(whole, weight) for weight in weights_list], axis=1)
    arrived = lax.all_to_all(packed, "kv", split_axis=0, concat_axis=0, tiled=True)
    groups = lax.axis_size("kv")
    seq_count = whole.shape[0] // groups
    local_heads = query_weight.shape[1]
    unpacked = []
    start = 0
    for weight in weights_list:
        channels = weight.shape[2]
        width = local_heads * channels
        block = arrived[:, start : start + width].reshape(groups, seq_count, local_heads, channels)
        block = block.transpose(1, 2, 0, 3).reshape(seq_count, local_heads, groups * channels)
        unpacked.append(block.astype(jnp.float32))
        start = start + width
    query_rows = unpacked[0] * KEY_DIM ** (-0.5)
    key_rows = unpacked[1]
    decay_rows = unpacked[2]
    value_rows = unpacked[3]
    gate_rows = unpacked[4]
    retain = jnp.exp(jax.nn.log_sigmoid(decay_rows + decay_bias) / TAU)
    new_states = retain[..., None] * states + key_rows[..., :, None] * value_rows[..., None, :]
    readout = jnp.einsum("shk,shkv->shv", query_rows, new_states, precision=lax.Precision.HIGHEST)
    readout = (
        readout
        * lax.rsqrt(jnp.mean(readout * readout, axis=-1, keepdims=True) + RMS_EPS)
        * head_gain
    )
    attended = (readout * jax.nn.silu(gate_rows)).astype(jnp.bfloat16)
    seq_count, local_heads, value_width = attended.shape
    flat_width = local_heads * value_width
    collected = lax.all_gather(
        attended.reshape(1, seq_count, flat_width), ("kv", "tp"), axis=0, tiled=True
    )
    halves = lax.axis_size("tp")
    collected = collected.reshape(-1, halves, seq_count, flat_width)
    columns = out_weight.shape[1]
    out_parts = out_weight.reshape(halves, flat_width, columns)
    mixed_heads = jnp.einsum(
        "atsc,tcd->asd", collected, out_parts, preferred_element_type=jnp.float32
    ).reshape(-1, columns)
    residual_one = ALPHA * tokens.astype(jnp.float32) + mixed_heads
    offset = lax.axis_index(("kv", "tp")) * columns
    totals = lax.psum(
        (
            jnp.sum(residual_one, axis=-1, keepdims=True),
            jnp.sum(residual_one * residual_one, axis=-1, keepdims=True),
        ),
        ("kv", "tp"),
    )
    average = totals[0] / D
    spread = totals[1] / D - average * average
    normed_own = normalize(residual_one, average, spread, norm1_gain, norm1_bias)
    normed = lax.all_gather(normed_own, ("kv", "tp"), axis=1, tiled=True)
    lifted = jnp.dot(normed, up_weight, preferred_element_type=jnp.float32)
    hidden = jnp.square(jax.nn.relu(lifted)).astype(jnp.bfloat16)
    mixer_term = jnp.dot(hidden, down_weight, preferred_element_type=jnp.float32)
    mixer_all = lax.psum(mixer_term, ("kv", "tp"))
    residual_two = ALPHA * normed.astype(jnp.float32) + mixer_all
    average = jnp.sum(residual_two, axis=-1, keepdims=True) / D
    spread = jnp.sum(residual_two * residual_two, axis=-1, keepdims=True) / D - average * average
    own_rows = lax.dynamic_slice_in_dim(residual_two, offset, columns, 1)
    layer_out = normalize(own_rows, average, spread, norm2_gain, norm2_bias)
    return (layer_out, new_states)


MESH = pl.DeviceIdType.MESH
F32 = jnp.float32
BF16 = jnp.bfloat16


def dot_nt(left, right):
    return lax.dot_general(left, right, (((1,), (1,)), ((), ())), preferred_element_type=F32)


def nearest(place, count, step, lower):
    below, above = place, count - 1 - place
    pairs = jnp.minimum(below, above)
    away = (step + 1) // 2 * (1 if step % 2 else -1)
    zigzag = jnp.where(lower, place - away, place + away)
    onward = jnp.where(below < above, place + (step - pairs), place - (step - pairs))
    return jnp.where(step <= 2 * pairs, zigzag, onward)


def layer_kernel(
    groups, halves, tokens, wq, wk, wd, wv, wg, bias, states, head_gain, wout, gain1, shift1,
    wup, wdown, gain2, shift2,
    out, states_out,
    proj_v, out_v, up_v, down_v, state_v, bias_v, hgain_v, gain1_v, shift1_v, gain2_v, shift2_v,
    bias_rows, x_v, acc_v, a_send, a_recv, a_rows, att_send, att_recv, x_rows, mixed_v, const_v, u_v, moments_v, both_v,
    p_send, p_recv, finals_v,
    load_sem, proj_sem, up_sem, down_sem, ready, own_ss, x_rs, a_ss, a_rs, c_ss, c_rs, t_ss, t_rs,
    u_ss, u_rs, m_ss, m_rs, p_ss, p_rs, f_ss, f_rs,
):
    my_kv, my_tp = lax.axis_index("kv"), lax.axis_index("tp")
    me = my_kv * halves + my_tp
    members, rows, cols = x_v.shape
    width = members * cols
    span = halves * cols
    seqs = rows // groups
    heads, kdim = bias_v.shape
    vdim = hgain_v.shape[1]
    kc, vc = kdim // groups, vdim // groups
    nk, nv = heads * kc, heads * vc
    top = groups - 1
    low_half = 2 * my_kv <= top
    rising = [nearest(my_kv, groups, step, my_kv >= 0) for step in range(groups)]
    chips = [nearest(my_kv, groups, step, low_half) for step in range(groups)]
    inward = [nearest(my_kv, groups, step, jnp.logical_not(low_half)) for step in range(groups)]
    cores = [lax.rem(my_tp + o, halves) for o in range(halves)]

    def load(src, dst, sem):
        copy = pltpu.make_async_copy(src, dst, sem)
        copy.start()
        return copy

    def chunk(chip):
        return pl.ds(pl.multiple_of(chip * span, span), span)

    loads = {}
    for index, (name, src, dst) in enumerate((
        ("tok", tokens, x_v.at[me]), ("g1", gain1, gain1_v), ("s1", shift1, shift1_v), ("bias", bias, bias_v),
    )):
        loads[name] = load(src, dst, load_sem.at[index])

    proj_loads = []

    def load_projections(step, chip):
        start = 0
        for index, weight in enumerate((wq, wk, wd, wv, wg)):
            size = weight.shape[0]
            proj_loads.append(load(
                weight.at[:, chunk(chip)], proj_v.at[pl.ds(start, size), chunk(chip)], proj_sem.at[step, index]
            ))
            start += size

    load_projections(0, rising[0])
    barrier = pltpu.get_barrier_semaphore()

    def greet(kv, tp):
        pl.semaphore_signal(barrier, inc=1, device_id={"kv": kv, "tp": tp}, device_id_type=MESH)

    @pl.when(my_kv > 0)
    def _():
        for core in cores:
            greet(my_kv - 1, core)

    for core in cores[1:]:
        greet(my_kv, core)
    for d in range(2, groups):

        @pl.when(my_kv + d < groups)
        def _():
            for core in cores:
                greet(my_kv + d, core)

    def remote(src, dst, send, recv, kv, tp):
        return pltpu.make_async_remote_copy(
            src_ref=src, dst_ref=dst, send_sem=send, recv_sem=recv, device_id={"kv": kv, "tp": tp},
            device_id_type=MESH,
        )

    def own_copy(kv, core, slot):
        return remote(x_v.at[me], x_v.at[me], own_ss.at[slot], x_rs.at[me], kv, core)

    def own_sends(first):
        plans = []
        if first:
            for o, core in enumerate(cores):
                plans.append((my_kv < top, my_kv + 1, core, o))
            for d in range(top, 1, -1):
                for o, core in enumerate(cores):
                    plans.append((my_kv >= d, my_kv - d, core, (d + 1) * halves + o))
            for o, core in enumerate(cores[1:]):
                plans.append((None, my_kv, core, halves + o))
        else:
            for o, core in enumerate(cores):
                plans.append((my_kv > 0, my_kv - 1, core, 2 * halves + o))
            for d in range(2, groups):
                for o, core in enumerate(cores):
                    plans.append((my_kv + d < groups, my_kv + d, core, (groups + d - 1) * halves + o))
        return plans

    def each_own(first, act):
        for condition, kv, core, slot in own_sends(first):
            if condition is None:
                act(own_copy(kv, core, slot))
            else:

                @pl.when(condition)
                def _():
                    act(own_copy(kv, core, slot))

    def send_below():
        pl.semaphore_wait(ready.at[1], halves)
        for o, core in enumerate(cores):
            own_copy(my_kv - 1, core, 2 * halves + o).start()

    def send_far():
        for d in range(top, 1, -1):

            @pl.when(my_kv + d < groups)
            def _():
                pl.semaphore_wait(ready.at[d], halves)
                for o, core in enumerate(cores):
                    own_copy(my_kv + d, core, (groups + d - 1) * halves + o).start()

    expected = (halves - 1) + halves * jnp.maximum(my_kv - 1, 0) + jnp.where(my_kv < top, halves, 0)
    pl.semaphore_wait(barrier, expected)
    for d in range(2, groups):

        @pl.when(my_kv >= d)
        def _():
            for core in cores:
                pl.semaphore_signal(
                    ready.at[d], inc=1, device_id={"kv": my_kv - d, "tp": core}, device_id_type=MESH
                )

    @pl.when(my_kv < top)
    def _():
        for core in cores:
            pl.semaphore_signal(
                ready.at[1], inc=1, device_id={"kv": my_kv + 1, "tp": core}, device_id_type=MESH
            )

    loads["tok"].wait()
    each_own(True, lambda copy: copy.start())
    load_projections(1, rising[1])

    @pl.when(my_kv > 0)
    def _():
        send_below()

    pending = []

    def everyone():
        targets = [(chip, core) for chip in reversed(chips[1:]) for core in range(halves)]
        return targets + [(my_kv, core) for core in cores[1:]]

    def near_first():
        targets = [(chip, core) for chip in inward[1:] for core in range(halves)]
        return [(my_kv, core) for core in cores[1:]] + targets

    def spread(buffer, send, recv, targets=None):
        for o, (chip, core) in enumerate(targets or everyone()):
            copy = remote(buffer.at[me], buffer.at[me], send.at[o], recv.at[me], chip, core)
            copy.start()
            pending.append(copy)

    def collect(buffer, recv, chip, core):
        block = chip * halves + core
        remote(buffer.at[block], buffer.at[block], recv.at[block], recv.at[block], my_kv, my_tp).wait_recv()

    late = []
    for step, chip in enumerate(rising):
        for core in cores if step else cores[1:]:
            collect(x_v, x_rs, chip, core)
        for index in range(5):
            proj_loads[step * 5 + index].wait()
        if step + 2 < groups:
            load_projections(step + 2, rising[step + 2])
        if step == max(groups - 2, 0):
            for index, (name, src, dst) in enumerate((
                ("hg", head_gain, hgain_v), ("g2", gain2, gain2_v), ("s2", shift2, shift2_v),
                ("st", states, state_v), ("out", wout, out_v),
            )):
                loads[name] = load(src, dst, load_sem.at[4 + index])
        if step == groups - 1:
            for index, to in enumerate(inward):
                late.append(load(wup.at[chunk(to), :], up_v.at[chunk(to), :], up_sem.at[index]))

        if step == 0:

            @pl.when(my_kv > 0)
            def _():
                send_far()

        @pl.when(my_kv >= 0)
        def _():
            blocks = x_v[pl.ds(chip * halves, halves)]
            left = jnp.concatenate([blocks[o] for o in range(halves)], axis=1)
            term = dot_nt(left, proj_v[:, chunk(chip)])
            acc_v[...] = acc_v[...] + term if step else term

        if step == 0:

            @pl.when(my_kv == 0)
            def _():
                send_far()

            loads["g1"].wait()
            loads["s1"].wait()
            loads["bias"].wait()
            whole_shift = shift1_v[...]
            coarse = whole_shift.astype(BF16).astype(F32)
            place = lax.broadcasted_iota(jnp.int32, (rows, cols), 0)
            consts = jnp.where(place == my_tp, gain1_v[...], 0.0)
            consts = jnp.where(place == halves, coarse, consts)
            consts = jnp.where(place == halves + 1, whole_shift - coarse, consts)
            const_v[me] = consts.astype(BF16)
            for h in range(heads):
                for b in range(groups):
                    piece = jnp.broadcast_to(bias_v[h : h + 1, b * kc : (b + 1) * kc], (seqs, kc))
                    bias_rows[b, :, h * kc : (h + 1) * kc] = piece
        if step == groups - 2:
            spread(const_v, c_ss, c_rs)
    quarter = down_v.shape[0] // 4
    down_loads = [
        load(wdown.at[pl.ds(i * quarter, quarter)], down_v.at[pl.ds(i * quarter, quarter)], down_sem.at[i])
        for i in range(4)
    ]

    for a in range(groups):
        a_send[a] = acc_v[a * seqs : (a + 1) * seqs, :].astype(BF16)
    for o, peer in enumerate(reversed(chips[1:])):
        copy = remote(a_send.at[peer], a_recv.at[my_kv], a_ss.at[o], a_rs.at[my_kv], peer, my_tp)
        copy.start()
        pending.append(copy)
    a_recv[my_kv] = a_send[my_kv]
    loads["st"].wait()
    loads["hg"].wait()
    def decay(z):
        return jnp.exp((jnp.minimum(z, 0.0) - jnp.log1p(jnp.exp(-jnp.abs(z)))) / TAU)

    totals = [[None] * heads for _ in range(seqs)]
    strength = None
    for step, peer in enumerate(chips):
        if step:
            remote(a_send.at[peer], a_recv.at[peer], a_ss.at[0], a_rs.at[peer], my_kv, my_tp).wait_recv()
        got = a_recv[peer].astype(F32)
        q = got[:, 0:nk] * KEY_DIM ** (-0.5)
        turned = jnp.concatenate(
            [q * decay(got[:, 2 * nk : 3 * nk] + bias_rows[peer]), q * got[:, nk : 2 * nk]], axis=1
        ).T
        met = jnp.concatenate(
            [jnp.sum(turned[nk + h * kc : nk + (h + 1) * kc, :], axis=0, keepdims=True) for h in range(heads)],
            axis=0,
        )
        strength = met if strength is None else strength + met
        for s in range(seqs):
            column = jnp.broadcast_to(turned[0:nk, s : s + 1], (nk, 128))
            for h in range(heads):
                for low in range(0, kc, 8):
                    block = state_v[s, h, pl.ds(pl.multiple_of(peer * kc + low, 8), 8), :]
                    part = column[h * kc + low : h * kc + low + 8]
                    term = jnp.concatenate([part] * (vdim // 128), axis=1) * block
                    totals[s][h] = term if totals[s][h] is None else totals[s][h] + term
    for b in range(groups):
        a_rows[b * seqs : (b + 1) * seqs, :] = a_recv[b].astype(F32)

    def wide(s, h, first):
        start = first + h * vc
        parts = [a_rows[b * seqs + s : b * seqs + s + 1, start : start + vc] for b in range(groups)]
        return jnp.concatenate(parts, axis=1)

    values = []
    for s in range(seqs):
        value = jnp.concatenate([wide(s, h, 3 * nk) for h in range(heads)], axis=0)
        gate = jnp.concatenate([wide(s, h, 3 * nk + nv) for h in range(heads)], axis=0)
        values.append(value)
        lines = [jnp.sum(total, axis=0, keepdims=True) for total in totals[s]]
        readout = jnp.concatenate(lines, axis=0) + strength[:, s : s + 1] * value
        power = jnp.mean(readout * readout, axis=-1, keepdims=True)
        readout = readout * lax.rsqrt(power + RMS_EPS) * hgain_v[...]
        attended = readout * (gate / (1.0 + jnp.exp(-gate)))
        for h in range(heads):
            att_send[s : s + 1, h * vdim : (h + 1) * vdim] = attended[h : h + 1, :].astype(BF16)
    for o, (chip, core) in enumerate(everyone()):
        copy = remote(att_send, att_recv.at[me], t_ss.at[o], t_rs.at[me], chip, core)
        copy.start()
        pending.append(copy)
    att_recv[me] = att_send[...]

    slopes = jnp.concatenate([bias_rows[b] for b in range(groups)], axis=0)
    retain = decay(a_rows[:, 2 * nk : 3 * nk] + slopes)
    later = jnp.concatenate([retain, a_rows[:, nk : 2 * nk]], axis=1).T
    for s in range(seqs):
        for h in range(heads):
            for b in range(groups):
                lane = b * seqs + s
                subs = slice(h * kc, (h + 1) * kc)
                keys = slice(nk + h * kc, nk + (h + 1) * kc)
                states_out[s, h, b * kc : (b + 1) * kc, :] = (
                    later[subs, lane : lane + 1] * state_v[s, h, b * kc : (b + 1) * kc, :]
                    + later[keys, lane : lane + 1] * values[s][h : h + 1, :]
                )

    half = heads * vdim

    loads["out"].wait()
    for step, chip in enumerate(chips):
        for core in cores if step else cores[1:]:
            collect(att_recv, t_rs, chip, core)
        for t in range(halves):
            x_rows[step * seqs : (step + 1) * seqs, t * half : (t + 1) * half] = att_recv[chip * halves + t]

    @pl.when(my_kv >= 0)
    def _():
        mixed = jnp.dot(x_rows[...], out_v[...], preferred_element_type=F32)
        for step, chip in enumerate(chips):
            mixed_v[chip] = mixed[step * seqs : (step + 1) * seqs]

    mixed = jnp.concatenate([mixed_v[a] for a in range(groups)], axis=0)
    residual = ALPHA * x_v[me].astype(F32) + mixed

    lane = lax.broadcasted_iota(jnp.int32, (rows, 128), 1)
    line = lax.broadcasted_iota(jnp.int32, (rows, 128), 0)

    def moments(block):
        center = jnp.sum(block, axis=-1, keepdims=True) / cols
        moved = block - center
        return center, moved, jnp.sum(moved * moved, axis=-1, keepdims=True)

    def as_row(center, power):
        both = jnp.where(lane == line, center, 0.0) + jnp.where(lane == line + rows, power, 0.0)
        return jnp.sum(both, axis=0, keepdims=True)

    def as_columns(row):
        center = jnp.sum(jnp.where(lane == line, row, 0.0), axis=-1, keepdims=True)
        power = jnp.sum(jnp.where(lane == line + rows, row, 0.0), axis=-1, keepdims=True)
        return center, power

    def combine(pairs):
        average = sum(center for center, _ in pairs) / members
        powers = sum(power + cols * jnp.square(center - average) for center, power in pairs)
        return average, lax.rsqrt(powers / width + LN_EPS)

    center, moved, power = moments(residual)
    u_v[me] = (moved * gain1_v[...]).astype(BF16)
    moments_v[me] = as_row(center, power)
    spread(moments_v, m_ss, m_rs)
    spread(u_v, u_ss, u_rs, near_first())

    for step, chip in enumerate(chips):
        for core in cores if step else cores[1:]:
            collect(const_v, c_rs, chip, core)
    lifted = fixed = None
    pairs = []
    for step, chip in enumerate(inward):
        late[step].wait()
        for core in cores if step else cores[1:]:
            collect(u_v, u_rs, chip, core)
            collect(moments_v, m_rs, chip, core)
        left = []
        for o in range(halves):
            block = chip * halves + o
            left.append(jnp.concatenate([u_v[block], const_v[block]], axis=0))
            pairs.append(as_columns(moments_v[block]))
        term = jnp.dot(jnp.concatenate(left, axis=1), up_v[chunk(chip), :], preferred_element_type=F32)
        main, extra = term[:rows], term[rows:]
        for o in range(halves):
            main = main + pairs[step * halves + o][0] * extra[o : o + 1]
        lifted = main if lifted is None else lifted + main
        fixed = extra if fixed is None else fixed + extra
    average, scale = combine(pairs)
    slope = sum(fixed[o : o + 1] for o in range(halves))
    lifted = scale * (lifted - average * slope) + (fixed[halves : halves + 1] + fixed[halves + 1 : halves + 2])
    hidden = jnp.square(jnp.maximum(lifted, 0.0)).astype(BF16)
    normed = ((residual - average) * scale * gain1_v[...] + shift1_v[...]).astype(BF16)

    def block_of(chip, core):
        return pl.ds(pl.multiple_of((chip * halves + core) * cols, cols), cols)

    for copy in down_loads:
        copy.wait()
    def send_sum(o, value, chip, core):
        p_send[o] = value.astype(BF16)
        copy = remote(p_send.at[o], p_recv.at[me], p_ss.at[o], p_rs.at[me], chip, core)
        copy.start()
        pending.append(copy)

    for step in range(top, 0, -1):
        both = jnp.dot(hidden, down_v[:, chunk(chips[step])], preferred_element_type=F32)
        for core in range(halves):
            send_sum((top - step) * halves + core, both[:, core * cols : (core + 1) * cols], chips[step], core)
    both_v[...] = jnp.dot(hidden, down_v[:, chunk(my_kv)], preferred_element_type=F32)
    for o, core in enumerate(cores[1:]):
        send_sum(top * halves + o, both_v[:, block_of(0, core)], my_kv, core)
    total = both_v[:, block_of(0, my_tp)]
    total = total + ALPHA * normed.astype(F32)
    for chip, core in everyone():
        collect(p_recv, p_rs, chip, core)
        total = total + p_recv[chip * halves + core].astype(F32)
    center, moved, power = moments(total)
    finals_v[me] = as_row(center, power)
    spread(finals_v, f_ss, f_rs)
    pairs = [(center, power)]
    loads["g2"].wait()
    loads["s2"].wait()
    for chip, core in reversed(everyone()):
        collect(finals_v, f_rs, chip, core)
        pairs.append(as_columns(finals_v[chip * halves + core]))
    average, scale = combine(pairs)
    out[...] = ((total - average) * scale * gain2_v[...] + shift2_v[...]).astype(BF16)

    each_own(True, lambda copy: copy.wait_send())
    each_own(False, lambda copy: copy.wait_send())
    for copy in pending:
        copy.wait_send()


def finish_kernel(result, fresh, out, states_out, sems):
    puts = [
        pltpu.make_async_copy(fresh, states_out, sems.at[0]),
        pltpu.make_async_copy(result, out, sems.at[1]),
    ]
    for put in puts:
        put.start()
    for put in puts:
        put.wait()


def fused(groups, halves, *arrays):
    (tokens, wq, wk, wv, wg, wd, bias, states, head_gain, wout, gain1, shift1, wup, wdown, gain2,
     shift2) = arrays

    def flat(weight):
        return weight.transpose(1, 2, 0).reshape(-1, weight.shape[0])

    def row(vector):
        return vector.reshape(1, -1)

    rows, cols = tokens.shape
    members = groups * halves
    width = wq.shape[0]
    seqs, heads, kdim, vdim = states.shape
    proj = 3 * wq.shape[1] * wq.shape[2] + 2 * wv.shape[1] * wv.shape[2]
    vmem = pltpu.VMEM
    dma = pltpu.SemaphoreType.DMA
    anywhere = pl.BlockSpec(memory_space=pl.ANY)
    inside = pl.BlockSpec(memory_space=pltpu.VMEM)
    scratch = [
        vmem((proj, width), BF16),
        vmem(wout.shape, BF16),
        vmem(wup.shape, BF16),
        vmem(wdown.shape, BF16),
        vmem(states.shape, F32),
        vmem(bias.shape, F32),
        vmem(head_gain.shape, F32),
        vmem((1, cols), F32),
        vmem((1, cols), F32),
        vmem((1, cols), F32),
        vmem((1, cols), F32),
        vmem((groups, seqs, heads * kdim // groups), F32),
        vmem((members, rows, cols), BF16),
        vmem((rows, proj), F32),
        vmem((groups, seqs, proj), BF16),
        vmem((groups, seqs, proj), BF16),
        vmem((rows, proj), F32),
        vmem((seqs, heads * vdim), BF16),
        vmem((members, seqs, heads * vdim), BF16),
        vmem((rows, halves * heads * vdim), BF16),
        vmem((groups, seqs, cols), F32),
        vmem((members, rows, cols), BF16),
        vmem((members, rows, cols), BF16),
        vmem((members, 1, 128), F32),
        vmem((rows, halves * cols), F32),
        vmem((members - 1, rows, cols), BF16),
        vmem((members, rows, cols), BF16),
        vmem((members, 1, 128), F32),
        dma((9,)),
        dma((groups, 5)),
        dma((groups,)),
        dma((4,)),
        pltpu.SemaphoreType.REGULAR((groups,)),
        dma((2 * groups * halves,)),
        dma((members,)),
        dma((groups,)),
        dma((groups,)),
    ]
    scratch += [dma((members,))] * 12
    result, fresh = pl.pallas_call(
        functools.partial(layer_kernel, groups, halves),
        out_shape=(
            vmem(tokens.shape, BF16),
            vmem(states.shape, F32),
        ),
        in_specs=[anywhere] * 16,
        out_specs=(inside, inside),
        scratch_shapes=scratch,
        compiler_params=pltpu.CompilerParams(
            collective_id=0, has_side_effects=True, vmem_limit_bytes=58*1024*1024
        ),
    )(
        tokens, flat(wq), flat(wk), flat(wd), flat(wv), flat(wg), bias, states, head_gain, wout,
        row(gain1), row(shift1), wup, wdown, row(gain2), row(shift2),
    )
    return pl.pallas_call(
        finish_kernel,
        out_shape=(
            jax.ShapeDtypeStruct(tokens.shape, BF16),
            jax.ShapeDtypeStruct(states.shape, F32),
        ),
        in_specs=[anywhere] * 2,
        out_specs=(anywhere, anywhere),
        scratch_shapes=[dma((2,))],
        compiler_params=pltpu.CompilerParams(vmem_limit_bytes=1048576),
    )(result, fresh)


def dispatch(groups, halves, *arrays):
    rows, cols = arrays[0].shape
    if rows == 8 and cols % 128 == 0 and rows % groups == 0 and groups > 2 and halves <= 4:
        return fused(groups, halves, *arrays)
    return body(*arrays)


def solution(mesh):
    placed = (
        P("dp", ("kv", "tp")),
        P(None, "tp", "kv"),
        P(None, "tp", "kv"),
        P(None, "tp", "kv"),
        P(None, "tp", "kv"),
        P(None, "tp", "kv"),
        P("tp", None),
        P(("dp", "kv"), "tp", None, None),
        P("tp", None),
        P(None, ("kv", "tp")),
        P(("kv", "tp")),
        P(("kv", "tp")),
        P(None, ("kv", "tp")),
        P(("kv", "tp"), None),
        P(("kv", "tp")),
        P(("kv", "tp")),
    )
    return jax.shard_map(
        functools.partial(dispatch, mesh.shape["kv"], mesh.shape["tp"]),
        mesh=mesh,
        in_specs=placed,
        out_specs=(P("dp", ("kv", "tp")), P(("dp", "kv"), "tp", None, None)),
        check_vma=False,
    )
```

```python
import functools

import jax
import jax.numpy as jnp
from jax import lax
from jax.experimental import pallas as pl
from jax.experimental.pallas import tpu as pltpu
from jax.sharding import PartitionSpec as P

D = 4096
KEY_DIM = 128


ALPHA = 2.0**0.5
TAU = 16.0
LN_EPS = 1e-05
RMS_EPS = 1e-06


def project_flat(inputs, weight):
    flattened = weight.reshape(weight.shape[0], -1)
    return jnp.dot(inputs, flattened, preferred_element_type=jnp.float32).astype(jnp.bfloat16)


def normalize(inputs, average, spread, row_gain, row_shift):
    return ((inputs - average) * lax.rsqrt(spread + LN_EPS) * row_gain + row_shift).astype(
        jnp.bfloat16
    )


def body(
    tokens,
    query_weight,
    key_weight,
    value_weight,
    gate_weight,
    decay_weight,
    decay_bias,
    states,
    head_gain,
    out_weight,
    norm1_gain,
    norm1_bias,
    up_weight,
    down_weight,
    norm2_gain,
    norm2_bias,
):
    whole = lax.all_gather(tokens, ("kv", "tp"), axis=1, tiled=True)
    weights_list = (query_weight, key_weight, decay_weight, value_weight, gate_weight)
    packed = jnp.concatenate([project_flat(whole, weight) for weight in weights_list], axis=1)
    arrived = lax.all_to_all(packed, "kv", split_axis=0, concat_axis=0, tiled=True)
    groups = lax.axis_size("kv")
    seq_count = whole.shape[0] // groups
    local_heads = query_weight.shape[1]
    unpacked = []
    start = 0
    for weight in weights_list:
        channels = weight.shape[2]
        width = local_heads * channels
        block = arrived[:, start : start + width].reshape(groups, seq_count, local_heads, channels)
        block = block.transpose(1, 2, 0, 3).reshape(seq_count, local_heads, groups * channels)
        unpacked.append(block.astype(jnp.float32))
        start = start + width
    query_rows = unpacked[0] * KEY_DIM ** (-0.5)
    key_rows = unpacked[1]
    decay_rows = unpacked[2]
    value_rows = unpacked[3]
    gate_rows = unpacked[4]
    retain = jnp.exp(jax.nn.log_sigmoid(decay_rows + decay_bias) / TAU)
    new_states = retain[..., None] * states + key_rows[..., :, None] * value_rows[..., None, :]
    readout = jnp.einsum("shk,shkv->shv", query_rows, new_states, precision=lax.Precision.HIGHEST)
    readout = (
        readout
        * lax.rsqrt(jnp.mean(readout * readout, axis=-1, keepdims=True) + RMS_EPS)
        * head_gain
    )
    attended = (readout * jax.nn.silu(gate_rows)).astype(jnp.bfloat16)
    seq_count, local_heads, value_width = attended.shape
    flat_width = local_heads * value_width
    collected = lax.all_gather(
        attended.reshape(1, seq_count, flat_width), ("kv", "tp"), axis=0, tiled=True
    )
    halves = lax.axis_size("tp")
    collected = collected.reshape(-1, halves, seq_count, flat_width)
    columns = out_weight.shape[1]
    out_parts = out_weight.reshape(halves, flat_width, columns)
    mixed_heads = jnp.einsum(
        "atsc,tcd->asd", collected, out_parts, preferred_element_type=jnp.float32
    ).reshape(-1, columns)
    residual_one = ALPHA * tokens.astype(jnp.float32) + mixed_heads
    offset = lax.axis_index(("kv", "tp")) * columns
    totals = lax.psum(
        (
            jnp.sum(residual_one, axis=-1, keepdims=True),
            jnp.sum(residual_one * residual_one, axis=-1, keepdims=True),
        ),
        ("kv", "tp"),
    )
    average = totals[0] / D
    spread = totals[1] / D - average * average
    normed_own = normalize(residual_one, average, spread, norm1_gain, norm1_bias)
    normed = lax.all_gather(normed_own, ("kv", "tp"), axis=1, tiled=True)
    lifted = jnp.dot(normed, up_weight, preferred_element_type=jnp.float32)
    hidden = jnp.square(jax.nn.relu(lifted)).astype(jnp.bfloat16)
    mixer_term = jnp.dot(hidden, down_weight, preferred_element_type=jnp.float32)
    mixer_all = lax.psum(mixer_term, ("kv", "tp"))
    residual_two = ALPHA * normed.astype(jnp.float32) + mixer_all
    average = jnp.sum(residual_two, axis=-1, keepdims=True) / D
    spread = jnp.sum(residual_two * residual_two, axis=-1, keepdims=True) / D - average * average
    own_rows = lax.dynamic_slice_in_dim(residual_two, offset, columns, 1)
    layer_out = normalize(own_rows, average, spread, norm2_gain, norm2_bias)
    return (layer_out, new_states)


MESH = pl.DeviceIdType.MESH
F32 = jnp.float32
BF16 = jnp.bfloat16


def dot_nt(left, right):
    return lax.dot_general(left, right, (((1,), (1,)), ((), ())), preferred_element_type=F32)


def nearest(place, count, step, lower):
    below, above = place, count - 1 - place
    pairs = jnp.minimum(below, above)
    away = (step + 1) // 2 * (1 if step % 2 else -1)
    zigzag = jnp.where(lower, place - away, place + away)
    onward = jnp.where(below < above, place + (step - pairs), place - (step - pairs))
    return jnp.where(step <= 2 * pairs, zigzag, onward)


def layer_kernel(
    groups, halves, tokens, wq, wk, wd, wv, wg, bias, states, head_gain, wout, gain1, shift1,
    wup, wdown, gain2, shift2,
    out, states_out,
    proj_v, out_v, up_v, down_v, state_v, bias_v, hgain_v, gain1_v, shift1_v, gain2_v, shift2_v,
    bias_rows, x_v, acc_v, a_send, a_recv, a_rows, att_send, att_recv, x_rows, mixed_v, const_v, u_v, moments_v, both_v,
    p_send, p_recv, finals_v,
    load_sem, proj_sem, up_sem, down_sem, ready, own_ss, x_rs, a_ss, a_rs, c_ss, c_rs, t_ss, t_rs,
    u_ss, u_rs, m_ss, m_rs, p_ss, p_rs, f_ss, f_rs,
):
    my_kv, my_tp = lax.axis_index("kv"), lax.axis_index("tp")
    me = my_kv * halves + my_tp
    members, rows, cols = x_v.shape
    width = members * cols
    span = halves * cols
    seqs = rows // groups
    heads, kdim = bias_v.shape
    vdim = hgain_v.shape[1]
    kc, vc = kdim // groups, vdim // groups
    nk, nv = heads * kc, heads * vc
    top = groups - 1
    low_half = 2 * my_kv <= top
    rising = [nearest(my_kv, groups, step, my_kv >= 0) for step in range(groups)]
    chips = [nearest(my_kv, groups, step, low_half) for step in range(groups)]
    inward = [nearest(my_kv, groups, step, jnp.logical_not(low_half)) for step in range(groups)]
    cores = [lax.rem(my_tp + o, halves) for o in range(halves)]

    def load(src, dst, sem):
        copy = pltpu.make_async_copy(src, dst, sem)
        copy.start()
        return copy

    def chunk(chip):
        return pl.ds(pl.multiple_of(chip * span, span), span)

    loads = {}
    for index, (name, src, dst) in enumerate((
        ("tok", tokens, x_v.at[me]), ("g1", gain1, gain1_v), ("s1", shift1, shift1_v), ("bias", bias, bias_v),
    )):
        loads[name] = load(src, dst, load_sem.at[index])

    proj_loads = []

    def load_projections(step, chip):
        start = 0
        for index, weight in enumerate((wq, wk, wd, wv, wg)):
            size = weight.shape[0]
            proj_loads.append(load(
                weight.at[:, chunk(chip)], proj_v.at[pl.ds(start, size), chunk(chip)], proj_sem.at[step, index]
            ))
            start += size

    load_projections(0, rising[0])
    barrier = pltpu.get_barrier_semaphore()

    def greet(kv, tp):
        pl.semaphore_signal(barrier, inc=1, device_id={"kv": kv, "tp": tp}, device_id_type=MESH)

    @pl.when(my_kv > 0)
    def _():
        for core in cores:
            greet(my_kv - 1, core)

    for core in cores[1:]:
        greet(my_kv, core)
    for d in range(2, groups):

        @pl.when(my_kv + d < groups)
        def _():
            for core in cores:
                greet(my_kv + d, core)

    def remote(src, dst, send, recv, kv, tp):
        return pltpu.make_async_remote_copy(
            src_ref=src, dst_ref=dst, send_sem=send, recv_sem=recv, device_id={"kv": kv, "tp": tp},
            device_id_type=MESH,
        )

    def own_copy(kv, core, slot):
        return remote(x_v.at[me], x_v.at[me], own_ss.at[slot], x_rs.at[me], kv, core)

    def own_sends(first):
        plans = []
        if first:
            for o, core in enumerate(cores):
                plans.append((my_kv < top, my_kv + 1, core, o))
            for d in range(top, 1, -1):
                for o, core in enumerate(cores):
                    plans.append((my_kv >= d, my_kv - d, core, (d + 1) * halves + o))
            for o, core in enumerate(cores[1:]):
                plans.append((None, my_kv, core, halves + o))
        else:
            for o, core in enumerate(cores):
                plans.append((my_kv > 0, my_kv - 1, core, 2 * halves + o))
            for d in range(2, groups):
                for o, core in enumerate(cores):
                    plans.append((my_kv + d < groups, my_kv + d, core, (groups + d - 1) * halves + o))
        return plans

    def each_own(first, act):
        for condition, kv, core, slot in own_sends(first):
            if condition is None:
                act(own_copy(kv, core, slot))
            else:

                @pl.when(condition)
                def _():
                    act(own_copy(kv, core, slot))

    def send_below():
        pl.semaphore_wait(ready.at[1], halves)
        for o, core in enumerate(cores):
            own_copy(my_kv - 1, core, 2 * halves + o).start()

    def send_far():
        for d in range(top, 1, -1):

            @pl.when(my_kv + d < groups)
            def _():
                pl.semaphore_wait(ready.at[d], halves)
                for o, core in enumerate(cores):
                    own_copy(my_kv + d, core, (groups + d - 1) * halves + o).start()

    expected = (halves - 1) + halves * jnp.maximum(my_kv - 1, 0) + jnp.where(my_kv < top, halves, 0)
    pl.semaphore_wait(barrier, expected)
    for d in range(2, groups):

        @pl.when(my_kv >= d)
        def _():
            for core in cores:
                pl.semaphore_signal(
                    ready.at[d], inc=1, device_id={"kv": my_kv - d, "tp": core}, device_id_type=MESH
                )

    @pl.when(my_kv < top)
    def _():
        for core in cores:
            pl.semaphore_signal(
                ready.at[1], inc=1, device_id={"kv": my_kv + 1, "tp": core}, device_id_type=MESH
            )

    loads["tok"].wait()
    each_own(True, lambda copy: copy.start())
    load_projections(1, rising[1])

    @pl.when(my_kv > 0)
    def _():
        send_below()

    pending = []

    def everyone():
        targets = [(chip, core) for chip in reversed(chips[1:]) for core in range(halves)]
        return targets + [(my_kv, core) for core in cores[1:]]

    def near_first():
        targets = [(chip, core) for chip in inward[1:] for core in range(halves)]
        return [(my_kv, core) for core in cores[1:]] + targets

    def spread(buffer, send, recv, targets=None):
        for o, (chip, core) in enumerate(targets or everyone()):
            copy = remote(buffer.at[me], buffer.at[me], send.at[o], recv.at[me], chip, core)
            copy.start()
            pending.append(copy)

    def collect(buffer, recv, chip, core):
        block = chip * halves + core
        remote(buffer.at[block], buffer.at[block], recv.at[block], recv.at[block], my_kv, my_tp).wait_recv()

    late = []
    for step, chip in enumerate(rising):
        for core in cores if step else cores[1:]:
            collect(x_v, x_rs, chip, core)
        for index in range(5):
            proj_loads[step * 5 + index].wait()
        if step + 2 < groups:
            load_projections(step + 2, rising[step + 2])
        if step == max(groups - 2, 0):
            for index, (name, src, dst) in enumerate((
                ("hg", head_gain, hgain_v), ("g2", gain2, gain2_v), ("s2", shift2, shift2_v),
                ("st", states, state_v), ("out", wout, out_v),
            )):
                loads[name] = load(src, dst, load_sem.at[4 + index])
        if step == groups - 1:
            for index, to in enumerate(inward):
                late.append(load(wup.at[chunk(to), :], up_v.at[chunk(to), :], up_sem.at[index]))

        if step == 0:

            @pl.when(my_kv > 0)
            def _():
                send_far()

        @pl.when(my_kv >= 0)
        def _():
            blocks = x_v[pl.ds(chip * halves, halves)]
            left = jnp.concatenate([blocks[o] for o in range(halves)], axis=1)
            term = dot_nt(left, proj_v[:, chunk(chip)])
            acc_v[...] = acc_v[...] + term if step else term

        if step == 0:

            @pl.when(my_kv == 0)
            def _():
                send_far()

            loads["g1"].wait()
            loads["s1"].wait()
            loads["bias"].wait()
            whole_shift = shift1_v[...]
            coarse = whole_shift.astype(BF16).astype(F32)
            place = lax.broadcasted_iota(jnp.int32, (rows, cols), 0)
            consts = jnp.where(place == my_tp, gain1_v[...], 0.0)
            consts = jnp.where(place == halves, coarse, consts)
            consts = jnp.where(place == halves + 1, whole_shift - coarse, consts)
            const_v[me] = consts.astype(BF16)
            for h in range(heads):
                for b in range(groups):
                    piece = jnp.broadcast_to(bias_v[h : h + 1, b * kc : (b + 1) * kc], (seqs, kc))
                    bias_rows[b, :, h * kc : (h + 1) * kc] = piece
        if step == groups - 2:
            spread(const_v, c_ss, c_rs)
    quarter = down_v.shape[0] // 4
    down_loads = [
        load(wdown.at[pl.ds(i * quarter, quarter)], down_v.at[pl.ds(i * quarter, quarter)], down_sem.at[i])
        for i in range(4)
    ]

    for a in range(groups):
        a_send[a] = acc_v[a * seqs : (a + 1) * seqs, :].astype(BF16)
    for o, peer in enumerate(reversed(chips[1:])):
        copy = remote(a_send.at[peer], a_recv.at[my_kv], a_ss.at[o], a_rs.at[my_kv], peer, my_tp)
        copy.start()
        pending.append(copy)
    a_recv[my_kv] = a_send[my_kv]
    loads["st"].wait()
    loads["hg"].wait()
    def decay(z):
        return jnp.exp((jnp.minimum(z, 0.0) - jnp.log1p(jnp.exp(-jnp.abs(z)))) / TAU)

    totals = [[None] * heads for _ in range(seqs)]
    strength = None
    for step, peer in enumerate(inward):
        if step:
            remote(a_send.at[peer], a_recv.at[peer], a_ss.at[0], a_rs.at[peer], my_kv, my_tp).wait_recv()
        got = a_recv[peer].astype(F32)
        q = got[:, 0:nk] * KEY_DIM ** (-0.5)
        turned = jnp.concatenate(
            [q * decay(got[:, 2 * nk : 3 * nk] + bias_rows[peer]), q * got[:, nk : 2 * nk]], axis=1
        ).T
        met = jnp.concatenate(
            [jnp.sum(turned[nk + h * kc : nk + (h + 1) * kc, :], axis=0, keepdims=True) for h in range(heads)],
            axis=0,
        )
        strength = met if strength is None else strength + met
        for s in range(seqs):
            column = jnp.broadcast_to(turned[0:nk, s : s + 1], (nk, 128))
            for h in range(heads):
                for low in range(0, kc, 8):
                    block = state_v[s, h, pl.ds(pl.multiple_of(peer * kc + low, 8), 8), :]
                    part = column[h * kc + low : h * kc + low + 8]
                    term = jnp.concatenate([part] * (vdim // 128), axis=1) * block
                    totals[s][h] = term if totals[s][h] is None else totals[s][h] + term
    for b in range(groups):
        a_rows[b * seqs : (b + 1) * seqs, :] = a_recv[b].astype(F32)

    def wide(s, h, first):
        start = first + h * vc
        parts = [a_rows[b * seqs + s : b * seqs + s + 1, start : start + vc] for b in range(groups)]
        return jnp.concatenate(parts, axis=1)

    values = []
    for s in range(seqs):
        value = jnp.concatenate([wide(s, h, 3 * nk) for h in range(heads)], axis=0)
        gate = jnp.concatenate([wide(s, h, 3 * nk + nv) for h in range(heads)], axis=0)
        values.append(value)
        lines = [jnp.sum(total, axis=0, keepdims=True) for total in totals[s]]
        readout = jnp.concatenate(lines, axis=0) + strength[:, s : s + 1] * value
        power = jnp.mean(readout * readout, axis=-1, keepdims=True)
        readout = readout * lax.rsqrt(power + RMS_EPS) * hgain_v[...]
        attended = readout * (gate / (1.0 + jnp.exp(-gate)))
        for h in range(heads):
            att_send[s : s + 1, h * vdim : (h + 1) * vdim] = attended[h : h + 1, :].astype(BF16)
    for o, (chip, core) in enumerate(everyone()):
        copy = remote(att_send, att_recv.at[me], t_ss.at[o], t_rs.at[me], chip, core)
        copy.start()
        pending.append(copy)
    att_recv[me] = att_send[...]

    slopes = jnp.concatenate([bias_rows[b] for b in range(groups)], axis=0)
    retain = decay(a_rows[:, 2 * nk : 3 * nk] + slopes)
    later = jnp.concatenate([retain, a_rows[:, nk : 2 * nk]], axis=1).T
    for s in range(seqs):
        for h in range(heads):
            for b in range(groups):
                lane = b * seqs + s
                subs = slice(h * kc, (h + 1) * kc)
                keys = slice(nk + h * kc, nk + (h + 1) * kc)
                states_out[s, h, b * kc : (b + 1) * kc, :] = (
                    later[subs, lane : lane + 1] * state_v[s, h, b * kc : (b + 1) * kc, :]
                    + later[keys, lane : lane + 1] * values[s][h : h + 1, :]
                )

    half = heads * vdim

    loads["out"].wait()
    for step, chip in enumerate(chips):
        for core in cores if step else cores[1:]:
            collect(att_recv, t_rs, chip, core)
        for t in range(halves):
            x_rows[step * seqs : (step + 1) * seqs, t * half : (t + 1) * half] = att_recv[chip * halves + t]

    @pl.when(my_kv >= 0)
    def _():
        mixed = jnp.dot(x_rows[...], out_v[...], preferred_element_type=F32)
        for step, chip in enumerate(chips):
            mixed_v[chip] = mixed[step * seqs : (step + 1) * seqs]

    mixed = jnp.concatenate([mixed_v[a] for a in range(groups)], axis=0)
    residual = ALPHA * x_v[me].astype(F32) + mixed

    lane = lax.broadcasted_iota(jnp.int32, (rows, 128), 1)
    line = lax.broadcasted_iota(jnp.int32, (rows, 128), 0)

    def as_row(center, power):
        both = jnp.where(lane == line, center, 0.0) + jnp.where(lane == line + rows, power, 0.0)
        return jnp.sum(both, axis=0, keepdims=True)

    def as_columns(row):
        center = jnp.sum(jnp.where(lane == line, row, 0.0), axis=-1, keepdims=True)
        power = jnp.sum(jnp.where(lane == line + rows, row, 0.0), axis=-1, keepdims=True)
        return center, power

    def combine(pairs):
        average = sum(center for center, _ in pairs) / members
        powers = sum(power + cols * jnp.square(center - average) for center, power in pairs)
        return average, lax.rsqrt(powers / width + LN_EPS)

    center = jnp.sum(residual, axis=-1, keepdims=True) / cols
    power = jnp.sum(residual * residual, axis=-1, keepdims=True) - cols * center * center
    u_v[me] = ((residual - center) * gain1_v[...]).astype(BF16)
    moments_v[me] = as_row(center, power)
    spread(moments_v, m_ss, m_rs)
    spread(u_v, u_ss, u_rs, near_first())

    for step, chip in enumerate(chips):
        for core in cores if step else cores[1:]:
            collect(const_v, c_rs, chip, core)
    lifted = fixed = None
    pairs = []
    for step, chip in enumerate(inward):
        late[step].wait()
        for core in cores if step else cores[1:]:
            collect(u_v, u_rs, chip, core)
            collect(moments_v, m_rs, chip, core)
        left = []
        for o in range(halves):
            block = chip * halves + o
            left.append(jnp.concatenate([u_v[block], const_v[block]], axis=0))
            pairs.append(as_columns(moments_v[block]))
        term = jnp.dot(jnp.concatenate(left, axis=1), up_v[chunk(chip), :], preferred_element_type=F32)
        main, extra = term[:rows], term[rows:]
        for o in range(halves):
            main = main + pairs[step * halves + o][0] * extra[o : o + 1]
        lifted = main if lifted is None else lifted + main
        fixed = extra if fixed is None else fixed + extra
    average, scale = combine(pairs)
    slope = sum(fixed[o : o + 1] for o in range(halves))
    lifted = scale * (lifted - average * slope) + (fixed[halves : halves + 1] + fixed[halves + 1 : halves + 2])
    hidden = jnp.square(jnp.maximum(lifted, 0.0)).astype(BF16)
    normed = ((residual - average) * scale * gain1_v[...] + shift1_v[...]).astype(BF16)

    def block_of(chip, core):
        return pl.ds(pl.multiple_of((chip * halves + core) * cols, cols), cols)

    for copy in down_loads:
        copy.wait()
    def send_sum(o, value, chip, core):
        p_send[o] = value.astype(BF16)
        copy = remote(p_send.at[o], p_recv.at[me], p_ss.at[o], p_rs.at[me], chip, core)
        copy.start()
        pending.append(copy)

    for step in range(top, 0, -1):
        both = jnp.dot(hidden, down_v[:, chunk(inward[step])], preferred_element_type=F32)
        for core in range(halves):
            send_sum((top - step) * halves + core, both[:, core * cols : (core + 1) * cols], inward[step], core)
    both_v[...] = jnp.dot(hidden, down_v[:, chunk(my_kv)], preferred_element_type=F32)
    for o, core in enumerate(cores[1:]):
        send_sum(top * halves + o, both_v[:, block_of(0, core)], my_kv, core)
    total = both_v[:, block_of(0, my_tp)]
    total = total + ALPHA * normed.astype(F32)
    for chip, core in everyone():
        collect(p_recv, p_rs, chip, core)
        total = total + p_recv[chip * halves + core].astype(F32)
    sums = jnp.sum(total, axis=-1, keepdims=True)
    squares = jnp.sum(total * total, axis=-1, keepdims=True)
    finals_v[me] = as_row(sums, squares)
    spread(finals_v, f_ss, f_rs)
    loads["g2"].wait()
    loads["s2"].wait()
    gathered = finals_v[me]
    for chip, core in reversed(everyone()):
        collect(finals_v, f_rs, chip, core)
        gathered = gathered + finals_v[chip * halves + core]
    sums, squares = as_columns(gathered)
    average = sums / width
    scale = lax.rsqrt(squares / width - average * average + LN_EPS)
    out[...] = ((total - average) * scale * gain2_v[...] + shift2_v[...]).astype(BF16)

    each_own(True, lambda copy: copy.wait_send())
    each_own(False, lambda copy: copy.wait_send())
    for copy in pending:
        copy.wait_send()


def finish_kernel(result, fresh, out, states_out, sems):
    puts = [
        pltpu.make_async_copy(fresh, states_out, sems.at[0]),
        pltpu.make_async_copy(result, out, sems.at[1]),
    ]
    for put in puts:
        put.start()
    for put in puts:
        put.wait()


def fused(groups, halves, *arrays):
    (tokens, wq, wk, wv, wg, wd, bias, states, head_gain, wout, gain1, shift1, wup, wdown, gain2,
     shift2) = arrays

    def flat(weight):
        return weight.transpose(1, 2, 0).reshape(-1, weight.shape[0])

    def row(vector):
        return vector.reshape(1, -1)

    rows, cols = tokens.shape
    members = groups * halves
    width = wq.shape[0]
    seqs, heads, kdim, vdim = states.shape
    proj = 3 * wq.shape[1] * wq.shape[2] + 2 * wv.shape[1] * wv.shape[2]
    vmem = pltpu.VMEM
    dma = pltpu.SemaphoreType.DMA
    anywhere = pl.BlockSpec(memory_space=pl.ANY)
    inside = pl.BlockSpec(memory_space=pltpu.VMEM)
    scratch = [
        vmem((proj, width), BF16),
        vmem(wout.shape, BF16),
        vmem(wup.shape, BF16),
        vmem(wdown.shape, BF16),
        vmem(states.shape, F32),
        vmem(bias.shape, F32),
        vmem(head_gain.shape, F32),
        vmem((1, cols), F32),
        vmem((1, cols), F32),
        vmem((1, cols), F32),
        vmem((1, cols), F32),
        vmem((groups, seqs, heads * kdim // groups), F32),
        vmem((members, rows, cols), BF16),
        vmem((rows, proj), F32),
        vmem((groups, seqs, proj), BF16),
        vmem((groups, seqs, proj), BF16),
        vmem((rows, proj), F32),
        vmem((seqs, heads * vdim), BF16),
        vmem((members, seqs, heads * vdim), BF16),
        vmem((rows, halves * heads * vdim), BF16),
        vmem((groups, seqs, cols), F32),
        vmem((members, rows, cols), BF16),
        vmem((members, rows, cols), BF16),
        vmem((members, 1, 128), F32),
        vmem((rows, halves * cols), F32),
        vmem((members - 1, rows, cols), BF16),
        vmem((members, rows, cols), BF16),
        vmem((members, 1, 128), F32),
        dma((9,)),
        dma((groups, 5)),
        dma((groups,)),
        dma((4,)),
        pltpu.SemaphoreType.REGULAR((groups,)),
        dma((2 * groups * halves,)),
        dma((members,)),
        dma((groups,)),
        dma((groups,)),
    ]
    scratch += [dma((members,))] * 12
    result, fresh = pl.pallas_call(
        functools.partial(layer_kernel, groups, halves),
        out_shape=(
            vmem(tokens.shape, BF16),
            vmem(states.shape, F32),
        ),
        in_specs=[anywhere] * 16,
        out_specs=(inside, inside),
        scratch_shapes=scratch,
        compiler_params=pltpu.CompilerParams(
            collective_id=0, has_side_effects=True, vmem_limit_bytes=58*1024*1024
        ),
    )(
        tokens, flat(wq), flat(wk), flat(wd), flat(wv), flat(wg), bias, states, head_gain, wout,
        row(gain1), row(shift1), wup, wdown, row(gain2), row(shift2),
    )
    return pl.pallas_call(
        finish_kernel,
        out_shape=(
            jax.ShapeDtypeStruct(tokens.shape, BF16),
            jax.ShapeDtypeStruct(states.shape, F32),
        ),
        in_specs=[anywhere] * 2,
        out_specs=(anywhere, anywhere),
        scratch_shapes=[dma((2,))],
        compiler_params=pltpu.CompilerParams(vmem_limit_bytes=1048576),
    )(result, fresh)


def dispatch(groups, halves, *arrays):
    rows, cols = arrays[0].shape
    if rows == 8 and cols % 128 == 0 and rows % groups == 0 and groups > 2 and halves <= 4:
        return fused(groups, halves, *arrays)
    return body(*arrays)


def solution(mesh):
    placed = (
        P("dp", ("kv", "tp")),
        P(None, "tp", "kv"),
        P(None, "tp", "kv"),
        P(None, "tp", "kv"),
        P(None, "tp", "kv"),
        P(None, "tp", "kv"),
        P("tp", None),
        P(("dp", "kv"), "tp", None, None),
        P("tp", None),
        P(None, ("kv", "tp")),
        P(("kv", "tp")),
        P(("kv", "tp")),
        P(None, ("kv", "tp")),
        P(("kv", "tp"), None),
        P(("kv", "tp")),
        P(("kv", "tp")),
    )
    return jax.shard_map(
        functools.partial(dispatch, mesh.shape["kv"], mesh.shape["tp"]),
        mesh=mesh,
        in_specs=placed,
        out_specs=(P("dp", ("kv", "tp")), P(("dp", "kv"), "tp", None, None)),
        check_vma=False,
    )
```

```python
import functools

import jax
import jax.numpy as jnp
from jax import lax
from jax.experimental import pallas as pl
from jax.experimental.pallas import tpu as pltpu
from jax.sharding import PartitionSpec as P

D = 4096
KEY_DIM = 128


ALPHA = 2.0**0.5
TAU = 16.0
LN_EPS = 1e-05
RMS_EPS = 1e-06


def project_flat(inputs, weight):
    flattened = weight.reshape(weight.shape[0], -1)
    return jnp.dot(inputs, flattened, preferred_element_type=jnp.float32).astype(jnp.bfloat16)


def normalize(inputs, average, spread, row_gain, row_shift):
    return ((inputs - average) * lax.rsqrt(spread + LN_EPS) * row_gain + row_shift).astype(
        jnp.bfloat16
    )


def body(
    tokens,
    query_weight,
    key_weight,
    value_weight,
    gate_weight,
    decay_weight,
    decay_bias,
    states,
    head_gain,
    out_weight,
    norm1_gain,
    norm1_bias,
    up_weight,
    down_weight,
    norm2_gain,
    norm2_bias,
):
    whole = lax.all_gather(tokens, ("kv", "tp"), axis=1, tiled=True)
    weights_list = (query_weight, key_weight, decay_weight, value_weight, gate_weight)
    packed = jnp.concatenate([project_flat(whole, weight) for weight in weights_list], axis=1)
    arrived = lax.all_to_all(packed, "kv", split_axis=0, concat_axis=0, tiled=True)
    groups = lax.axis_size("kv")
    seq_count = whole.shape[0] // groups
    local_heads = query_weight.shape[1]
    unpacked = []
    start = 0
    for weight in weights_list:
        channels = weight.shape[2]
        width = local_heads * channels
        block = arrived[:, start : start + width].reshape(groups, seq_count, local_heads, channels)
        block = block.transpose(1, 2, 0, 3).reshape(seq_count, local_heads, groups * channels)
        unpacked.append(block.astype(jnp.float32))
        start = start + width
    query_rows = unpacked[0] * KEY_DIM ** (-0.5)
    key_rows = unpacked[1]
    decay_rows = unpacked[2]
    value_rows = unpacked[3]
    gate_rows = unpacked[4]
    retain = jnp.exp(jax.nn.log_sigmoid(decay_rows + decay_bias) / TAU)
    new_states = retain[..., None] * states + key_rows[..., :, None] * value_rows[..., None, :]
    readout = jnp.einsum("shk,shkv->shv", query_rows, new_states, precision=lax.Precision.HIGHEST)
    readout = (
        readout
        * lax.rsqrt(jnp.mean(readout * readout, axis=-1, keepdims=True) + RMS_EPS)
        * head_gain
    )
    attended = (readout * jax.nn.silu(gate_rows)).astype(jnp.bfloat16)
    seq_count, local_heads, value_width = attended.shape
    flat_width = local_heads * value_width
    collected = lax.all_gather(
        attended.reshape(1, seq_count, flat_width), ("kv", "tp"), axis=0, tiled=True
    )
    halves = lax.axis_size("tp")
    collected = collected.reshape(-1, halves, seq_count, flat_width)
    columns = out_weight.shape[1]
    out_parts = out_weight.reshape(halves, flat_width, columns)
    mixed_heads = jnp.einsum(
        "atsc,tcd->asd", collected, out_parts, preferred_element_type=jnp.float32
    ).reshape(-1, columns)
    residual_one = ALPHA * tokens.astype(jnp.float32) + mixed_heads
    offset = lax.axis_index(("kv", "tp")) * columns
    totals = lax.psum(
        (
            jnp.sum(residual_one, axis=-1, keepdims=True),
            jnp.sum(residual_one * residual_one, axis=-1, keepdims=True),
        ),
        ("kv", "tp"),
    )
    average = totals[0] / D
    spread = totals[1] / D - average * average
    normed_own = normalize(residual_one, average, spread, norm1_gain, norm1_bias)
    normed = lax.all_gather(normed_own, ("kv", "tp"), axis=1, tiled=True)
    lifted = jnp.dot(normed, up_weight, preferred_element_type=jnp.float32)
    hidden = jnp.square(jax.nn.relu(lifted)).astype(jnp.bfloat16)
    mixer_term = jnp.dot(hidden, down_weight, preferred_element_type=jnp.float32)
    mixer_all = lax.psum(mixer_term, ("kv", "tp"))
    residual_two = ALPHA * normed.astype(jnp.float32) + mixer_all
    average = jnp.sum(residual_two, axis=-1, keepdims=True) / D
    spread = jnp.sum(residual_two * residual_two, axis=-1, keepdims=True) / D - average * average
    own_rows = lax.dynamic_slice_in_dim(residual_two, offset, columns, 1)
    layer_out = normalize(own_rows, average, spread, norm2_gain, norm2_bias)
    return (layer_out, new_states)


MESH = pl.DeviceIdType.MESH
F32 = jnp.float32
BF16 = jnp.bfloat16


def dot_nt(left, right):
    return lax.dot_general(left, right, (((1,), (1,)), ((), ())), preferred_element_type=F32)


def nearest(place, count, step, lower):
    below, above = place, count - 1 - place
    pairs = jnp.minimum(below, above)
    away = (step + 1) // 2 * (1 if step % 2 else -1)
    zigzag = jnp.where(lower, place - away, place + away)
    onward = jnp.where(below < above, place + (step - pairs), place - (step - pairs))
    return jnp.where(step <= 2 * pairs, zigzag, onward)


def layer_kernel(
    groups, halves, tokens, wq, wk, wd, wv, wg, bias, states, head_gain, wout, gain1, shift1,
    wup, wdown, gain2, shift2,
    out, states_out,
    proj_v, out_v, up_v, down_v, state_v, bias_v, hgain_v, gain1_v, shift1_v, gain2_v, shift2_v,
    bias_rows, x_v, acc_v, a_send, a_recv, a_rows, att_send, att_recv, x_rows, mixed_v, const_v, u_v, moments_v, both_v,
    p_send, p_recv, finals_v,
    load_sem, proj_sem, up_sem, down_sem, ready, own_ss, x_rs, a_ss, a_rs, c_ss, c_rs, t_ss, t_rs,
    u_ss, u_rs, m_ss, m_rs, p_ss, p_rs, f_ss, f_rs,
):
    my_kv, my_tp = lax.axis_index("kv"), lax.axis_index("tp")
    me = my_kv * halves + my_tp
    members, rows, cols = x_v.shape
    width = members * cols
    span = halves * cols
    seqs = rows // groups
    heads, kdim = bias_v.shape
    vdim = hgain_v.shape[1]
    kc, vc = kdim // groups, vdim // groups
    nk, nv = heads * kc, heads * vc
    top = groups - 1
    low_half = 2 * my_kv <= top
    rising = [nearest(my_kv, groups, step, my_kv >= 0) for step in range(groups)]
    chips = [nearest(my_kv, groups, step, low_half) for step in range(groups)]
    inward = [nearest(my_kv, groups, step, jnp.logical_not(low_half)) for step in range(groups)]
    cores = [lax.rem(my_tp + o, halves) for o in range(halves)]

    def load(src, dst, sem):
        copy = pltpu.make_async_copy(src, dst, sem)
        copy.start()
        return copy

    def chunk(chip):
        return pl.ds(pl.multiple_of(chip * span, span), span)

    loads = {}
    for index, (name, src, dst) in enumerate((
        ("tok", tokens, x_v.at[me]), ("g1", gain1, gain1_v), ("s1", shift1, shift1_v), ("bias", bias, bias_v),
    )):
        loads[name] = load(src, dst, load_sem.at[index])

    proj_loads = []

    def load_projections(step, chip):
        start = 0
        for index, weight in enumerate((wq, wk, wd, wv, wg)):
            size = weight.shape[0]
            proj_loads.append(load(
                weight.at[:, chunk(chip)], proj_v.at[pl.ds(start, size), chunk(chip)], proj_sem.at[step, index]
            ))
            start += size

    load_projections(0, rising[0])
    barrier = pltpu.get_barrier_semaphore()

    def greet(kv, tp):
        pl.semaphore_signal(barrier, inc=1, device_id={"kv": kv, "tp": tp}, device_id_type=MESH)

    @pl.when(my_kv > 0)
    def _():
        for core in cores:
            greet(my_kv - 1, core)

    for core in cores[1:]:
        greet(my_kv, core)
    for d in range(2, groups):

        @pl.when(my_kv + d < groups)
        def _():
            for core in cores:
                greet(my_kv + d, core)

    def remote(src, dst, send, recv, kv, tp):
        return pltpu.make_async_remote_copy(
            src_ref=src, dst_ref=dst, send_sem=send, recv_sem=recv, device_id={"kv": kv, "tp": tp},
            device_id_type=MESH,
        )

    def own_copy(kv, core, slot):
        return remote(x_v.at[me], x_v.at[me], own_ss.at[slot], x_rs.at[me], kv, core)

    def own_sends(first):
        plans = []
        if first:
            for o, core in enumerate(cores):
                plans.append((my_kv < top, my_kv + 1, core, o))
            for d in range(top, 1, -1):
                for o, core in enumerate(cores):
                    plans.append((my_kv >= d, my_kv - d, core, (d + 1) * halves + o))
            for o, core in enumerate(cores[1:]):
                plans.append((None, my_kv, core, halves + o))
        else:
            for o, core in enumerate(cores):
                plans.append((my_kv > 0, my_kv - 1, core, 2 * halves + o))
            for d in range(2, groups):
                for o, core in enumerate(cores):
                    plans.append((my_kv + d < groups, my_kv + d, core, (groups + d - 1) * halves + o))
        return plans

    def each_own(first, act):
        for condition, kv, core, slot in own_sends(first):
            if condition is None:
                act(own_copy(kv, core, slot))
            else:

                @pl.when(condition)
                def _():
                    act(own_copy(kv, core, slot))

    def send_below():
        pl.semaphore_wait(ready.at[1], halves)
        for o, core in enumerate(cores):
            own_copy(my_kv - 1, core, 2 * halves + o).start()

    def send_far():
        for d in range(top, 1, -1):

            @pl.when(my_kv + d < groups)
            def _():
                pl.semaphore_wait(ready.at[d], halves)
                for o, core in enumerate(cores):
                    own_copy(my_kv + d, core, (groups + d - 1) * halves + o).start()

    expected = (halves - 1) + halves * jnp.maximum(my_kv - 1, 0) + jnp.where(my_kv < top, halves, 0)
    pl.semaphore_wait(barrier, expected)
    for d in range(2, groups):

        @pl.when(my_kv >= d)
        def _():
            for core in cores:
                pl.semaphore_signal(
                    ready.at[d], inc=1, device_id={"kv": my_kv - d, "tp": core}, device_id_type=MESH
                )

    @pl.when(my_kv < top)
    def _():
        for core in cores:
            pl.semaphore_signal(
                ready.at[1], inc=1, device_id={"kv": my_kv + 1, "tp": core}, device_id_type=MESH
            )

    loads["tok"].wait()
    each_own(True, lambda copy: copy.start())
    load_projections(1, rising[1])

    @pl.when(my_kv > 0)
    def _():
        send_below()

    pending = []

    def everyone():
        targets = [(chip, core) for chip in reversed(chips[1:]) for core in range(halves)]
        return targets + [(my_kv, core) for core in cores[1:]]

    def near_first():
        targets = [(chip, core) for chip in inward[1:] for core in range(halves)]
        return [(my_kv, core) for core in cores[1:]] + targets

    def spread(buffer, send, recv, targets=None):
        for o, (chip, core) in enumerate(targets or everyone()):
            copy = remote(buffer.at[me], buffer.at[me], send.at[o], recv.at[me], chip, core)
            copy.start()
            pending.append(copy)

    def collect(buffer, recv, chip, core):
        block = chip * halves + core
        remote(buffer.at[block], buffer.at[block], recv.at[block], recv.at[block], my_kv, my_tp).wait_recv()

    late = []
    for step, chip in enumerate(rising):
        for core in cores if step else cores[1:]:
            collect(x_v, x_rs, chip, core)
        for index in range(5):
            proj_loads[step * 5 + index].wait()
        if step + 2 < groups:
            load_projections(step + 2, rising[step + 2])
        if step == max(groups - 2, 0):
            for index, (name, src, dst) in enumerate((
                ("hg", head_gain, hgain_v), ("g2", gain2, gain2_v), ("s2", shift2, shift2_v),
                ("st", states, state_v), ("out", wout, out_v),
            )):
                loads[name] = load(src, dst, load_sem.at[4 + index])
        if step == groups - 1:
            for index, to in enumerate(inward):
                late.append(load(wup.at[chunk(to), :], up_v.at[chunk(to), :], up_sem.at[index]))

        if step == 0:

            @pl.when(my_kv > 0)
            def _():
                send_far()

        @pl.when(my_kv >= 0)
        def _():
            blocks = x_v[pl.ds(chip * halves, halves)]
            left = jnp.concatenate([blocks[o] for o in range(halves)], axis=1)
            term = dot_nt(left, proj_v[:, chunk(chip)])
            acc_v[...] = acc_v[...] + term if step else term

        if step == 0:

            @pl.when(my_kv == 0)
            def _():
                send_far()

            loads["g1"].wait()
            loads["s1"].wait()
            loads["bias"].wait()
            whole_shift = shift1_v[...]
            coarse = whole_shift.astype(BF16).astype(F32)
            place = lax.broadcasted_iota(jnp.int32, (rows, cols), 0)
            consts = jnp.where(place == my_tp, gain1_v[...], 0.0)
            consts = jnp.where(place == halves, coarse, consts)
            consts = jnp.where(place == halves + 1, whole_shift - coarse, consts)
            const_v[me] = consts.astype(BF16)
            for h in range(heads):
                for b in range(groups):
                    piece = jnp.broadcast_to(bias_v[h : h + 1, b * kc : (b + 1) * kc], (seqs, kc))
                    bias_rows[b, :, h * kc : (h + 1) * kc] = piece
        if step == groups - 3:
            spread(const_v, c_ss, c_rs)
    quarter = down_v.shape[0] // 4
    down_loads = [
        load(wdown.at[pl.ds(i * quarter, quarter)], down_v.at[pl.ds(i * quarter, quarter)], down_sem.at[i])
        for i in range(4)
    ]

    for a in range(groups):
        a_send[a] = acc_v[a * seqs : (a + 1) * seqs, :].astype(BF16)
    for o, peer in enumerate(reversed(chips[1:])):
        copy = remote(a_send.at[peer], a_recv.at[my_kv], a_ss.at[o], a_rs.at[my_kv], peer, my_tp)
        copy.start()
        pending.append(copy)
    a_recv[my_kv] = a_send[my_kv]
    loads["st"].wait()
    loads["hg"].wait()
    def decay(z):
        return jnp.exp((jnp.minimum(z, 0.0) - jnp.log1p(jnp.exp(-jnp.abs(z)))) / TAU)

    totals = [[None] * heads for _ in range(seqs)]
    strength = None
    for step, peer in enumerate(inward):
        if step:
            remote(a_send.at[peer], a_recv.at[peer], a_ss.at[0], a_rs.at[peer], my_kv, my_tp).wait_recv()
        got = a_recv[peer].astype(F32)
        q = got[:, 0:nk] * KEY_DIM ** (-0.5)
        turned = jnp.concatenate(
            [q * decay(got[:, 2 * nk : 3 * nk] + bias_rows[peer]), q * got[:, nk : 2 * nk]], axis=1
        ).T
        met = jnp.concatenate(
            [jnp.sum(turned[nk + h * kc : nk + (h + 1) * kc, :], axis=0, keepdims=True) for h in range(heads)],
            axis=0,
        )
        strength = met if strength is None else strength + met
        for s in range(seqs):
            column = jnp.broadcast_to(turned[0:nk, s : s + 1], (nk, 128))
            for h in range(heads):
                for low in range(0, kc, 8):
                    block = state_v[s, h, pl.ds(pl.multiple_of(peer * kc + low, 8), 8), :]
                    part = column[h * kc + low : h * kc + low + 8]
                    term = jnp.concatenate([part] * (vdim // 128), axis=1) * block
                    totals[s][h] = term if totals[s][h] is None else totals[s][h] + term
    for b in range(groups):
        a_rows[b * seqs : (b + 1) * seqs, :] = a_recv[b].astype(F32)

    def wide(s, h, first):
        start = first + h * vc
        parts = [a_rows[b * seqs + s : b * seqs + s + 1, start : start + vc] for b in range(groups)]
        return jnp.concatenate(parts, axis=1)

    values = []
    for s in range(seqs):
        value = jnp.concatenate([wide(s, h, 3 * nk) for h in range(heads)], axis=0)
        gate = jnp.concatenate([wide(s, h, 3 * nk + nv) for h in range(heads)], axis=0)
        values.append(value)
        lines = [jnp.sum(total, axis=0, keepdims=True) for total in totals[s]]
        readout = jnp.concatenate(lines, axis=0) + strength[:, s : s + 1] * value
        power = jnp.mean(readout * readout, axis=-1, keepdims=True)
        readout = readout * lax.rsqrt(power + RMS_EPS) * hgain_v[...]
        attended = readout * (gate / (1.0 + jnp.exp(-gate)))
        for h in range(heads):
            att_send[s : s + 1, h * vdim : (h + 1) * vdim] = attended[h : h + 1, :].astype(BF16)
    for o, (chip, core) in enumerate(everyone()):
        copy = remote(att_send, att_recv.at[me], t_ss.at[o], t_rs.at[me], chip, core)
        copy.start()
        pending.append(copy)
    att_recv[me] = att_send[...]

    slopes = jnp.concatenate([bias_rows[b] for b in range(groups)], axis=0)
    retain = decay(a_rows[:, 2 * nk : 3 * nk] + slopes)
    later = jnp.concatenate([retain, a_rows[:, nk : 2 * nk]], axis=1).T
    for s in range(seqs):
        for h in range(heads):
            for b in range(groups):
                lane = b * seqs + s
                subs = slice(h * kc, (h + 1) * kc)
                keys = slice(nk + h * kc, nk + (h + 1) * kc)
                states_out[s, h, b * kc : (b + 1) * kc, :] = (
                    later[subs, lane : lane + 1] * state_v[s, h, b * kc : (b + 1) * kc, :]
                    + later[keys, lane : lane + 1] * values[s][h : h + 1, :]
                )

    half = heads * vdim

    loads["out"].wait()
    for step, chip in enumerate(chips):
        for core in cores if step else cores[1:]:
            collect(att_recv, t_rs, chip, core)
        for t in range(halves):
            x_rows[step * seqs : (step + 1) * seqs, t * half : (t + 1) * half] = att_recv[chip * halves + t]

    @pl.when(my_kv >= 0)
    def _():
        mixed = jnp.dot(x_rows[...], out_v[...], preferred_element_type=F32)
        for step, chip in enumerate(chips):
            mixed_v[chip] = mixed[step * seqs : (step + 1) * seqs]

    mixed = jnp.concatenate([mixed_v[a] for a in range(groups)], axis=0)
    residual = ALPHA * x_v[me].astype(F32) + mixed

    lane = lax.broadcasted_iota(jnp.int32, (rows, 128), 1)
    line = lax.broadcasted_iota(jnp.int32, (rows, 128), 0)

    def as_row(center, power):
        both = jnp.where(lane == line, center, 0.0) + jnp.where(lane == line + rows, power, 0.0)
        return jnp.sum(both, axis=0, keepdims=True)

    def as_columns(row):
        center = jnp.sum(jnp.where(lane == line, row, 0.0), axis=-1, keepdims=True)
        power = jnp.sum(jnp.where(lane == line + rows, row, 0.0), axis=-1, keepdims=True)
        return center, power

    def combine(pairs):
        average = sum(center for center, _ in pairs) / members
        powers = sum(power + cols * jnp.square(center - average) for center, power in pairs)
        return average, lax.rsqrt(powers / width + LN_EPS)

    center = jnp.sum(residual, axis=-1, keepdims=True) / cols
    power = jnp.sum(residual * residual, axis=-1, keepdims=True) - cols * center * center
    u_v[me] = ((residual - center) * gain1_v[...]).astype(BF16)
    moments_v[me] = as_row(center, power)
    spread(moments_v, m_ss, m_rs)
    spread(u_v, u_ss, u_rs, near_first())

    for step, chip in enumerate(chips):
        for core in cores if step else cores[1:]:
            collect(const_v, c_rs, chip, core)
    lifted = fixed = None
    pairs = []
    for step, chip in enumerate(inward):
        late[step].wait()
        for core in cores if step else cores[1:]:
            collect(u_v, u_rs, chip, core)
            collect(moments_v, m_rs, chip, core)
        left = []
        for o in range(halves):
            block = chip * halves + o
            left.append(jnp.concatenate([u_v[block], const_v[block]], axis=0))
            pairs.append(as_columns(moments_v[block]))
        term = jnp.dot(jnp.concatenate(left, axis=1), up_v[chunk(chip), :], preferred_element_type=F32)
        main, extra = term[:rows], term[rows:]
        for o in range(halves):
            main = main + pairs[step * halves + o][0] * extra[o : o + 1]
        lifted = main if lifted is None else lifted + main
        fixed = extra if fixed is None else fixed + extra
    average, scale = combine(pairs)
    slope = sum(fixed[o : o + 1] for o in range(halves))
    lifted = scale * (lifted - average * slope) + (fixed[halves : halves + 1] + fixed[halves + 1 : halves + 2])
    hidden = jnp.square(jnp.maximum(lifted, 0.0)).astype(BF16)
    normed = ((residual - average) * scale * gain1_v[...] + shift1_v[...]).astype(BF16)

    def block_of(chip, core):
        return pl.ds(pl.multiple_of((chip * halves + core) * cols, cols), cols)

    for copy in down_loads:
        copy.wait()
    def send_sum(o, value, chip, core):
        p_send[o] = value.astype(BF16)
        copy = remote(p_send.at[o], p_recv.at[me], p_ss.at[o], p_rs.at[me], chip, core)
        copy.start()
        pending.append(copy)

    for step in range(top, 0, -1):
        both = jnp.dot(hidden, down_v[:, chunk(inward[step])], preferred_element_type=F32)
        for core in range(halves):
            send_sum((top - step) * halves + core, both[:, core * cols : (core + 1) * cols], inward[step], core)
    for o, core in enumerate(cores[1:]):
        part = jnp.dot(hidden, down_v[:, block_of(my_kv, core)], preferred_element_type=F32)
        send_sum(top * halves + o, part, my_kv, core)
    total = jnp.dot(hidden, down_v[:, block_of(my_kv, my_tp)], preferred_element_type=F32)
    total = total + ALPHA * normed.astype(F32)
    for chip, core in everyone():
        collect(p_recv, p_rs, chip, core)
        total = total + p_recv[chip * halves + core].astype(F32)
    sums = jnp.sum(total, axis=-1, keepdims=True)
    squares = jnp.sum(total * total, axis=-1, keepdims=True)
    finals_v[me] = as_row(sums, squares)
    spread(finals_v, f_ss, f_rs)
    loads["g2"].wait()
    loads["s2"].wait()
    gathered = finals_v[me]
    for chip, core in reversed(everyone()):
        collect(finals_v, f_rs, chip, core)
        gathered = gathered + finals_v[chip * halves + core]
    sums, squares = as_columns(gathered)
    average = sums / width
    scale = lax.rsqrt(squares / width - average * average + LN_EPS)
    out[...] = ((total - average) * scale * gain2_v[...] + shift2_v[...]).astype(BF16)

    each_own(True, lambda copy: copy.wait_send())
    each_own(False, lambda copy: copy.wait_send())
    for copy in pending:
        copy.wait_send()


def finish_kernel(result, fresh, out, states_out, sems):
    puts = [
        pltpu.make_async_copy(fresh, states_out, sems.at[0]),
        pltpu.make_async_copy(result, out, sems.at[1]),
    ]
    for put in puts:
        put.start()
    for put in puts:
        put.wait()


def fused(groups, halves, *arrays):
    (tokens, wq, wk, wv, wg, wd, bias, states, head_gain, wout, gain1, shift1, wup, wdown, gain2,
     shift2) = arrays

    def flat(weight):
        return weight.transpose(1, 2, 0).reshape(-1, weight.shape[0])

    def row(vector):
        return vector.reshape(1, -1)

    rows, cols = tokens.shape
    members = groups * halves
    width = wq.shape[0]
    seqs, heads, kdim, vdim = states.shape
    proj = 3 * wq.shape[1] * wq.shape[2] + 2 * wv.shape[1] * wv.shape[2]
    vmem = pltpu.VMEM
    dma = pltpu.SemaphoreType.DMA
    anywhere = pl.BlockSpec(memory_space=pl.ANY)
    inside = pl.BlockSpec(memory_space=pltpu.VMEM)
    scratch = [
        vmem((proj, width), BF16),
        vmem(wout.shape, BF16),
        vmem(wup.shape, BF16),
        vmem(wdown.shape, BF16),
        vmem(states.shape, F32),
        vmem(bias.shape, F32),
        vmem(head_gain.shape, F32),
        vmem((1, cols), F32),
        vmem((1, cols), F32),
        vmem((1, cols), F32),
        vmem((1, cols), F32),
        vmem((groups, seqs, heads * kdim // groups), F32),
        vmem((members, rows, cols), BF16),
        vmem((rows, proj), F32),
        vmem((groups, seqs, proj), BF16),
        vmem((groups, seqs, proj), BF16),
        vmem((rows, proj), F32),
        vmem((seqs, heads * vdim), BF16),
        vmem((members, seqs, heads * vdim), BF16),
        vmem((rows, halves * heads * vdim), BF16),
        vmem((groups, seqs, cols), F32),
        vmem((members, rows, cols), BF16),
        vmem((members, rows, cols), BF16),
        vmem((members, 1, 128), F32),
        vmem((rows, halves * cols), F32),
        vmem((members - 1, rows, cols), BF16),
        vmem((members, rows, cols), BF16),
        vmem((members, 1, 128), F32),
        dma((9,)),
        dma((groups, 5)),
        dma((groups,)),
        dma((4,)),
        pltpu.SemaphoreType.REGULAR((groups,)),
        dma((2 * groups * halves,)),
        dma((members,)),
        dma((groups,)),
        dma((groups,)),
    ]
    scratch += [dma((members,))] * 12
    result, fresh = pl.pallas_call(
        functools.partial(layer_kernel, groups, halves),
        out_shape=(
            vmem(tokens.shape, BF16),
            vmem(states.shape, F32),
        ),
        in_specs=[anywhere] * 16,
        out_specs=(inside, inside),
        scratch_shapes=scratch,
        compiler_params=pltpu.CompilerParams(
            collective_id=0, has_side_effects=True, vmem_limit_bytes=58*1024*1024
        ),
    )(
        tokens, flat(wq), flat(wk), flat(wd), flat(wv), flat(wg), bias, states, head_gain, wout,
        row(gain1), row(shift1), wup, wdown, row(gain2), row(shift2),
    )
    return pl.pallas_call(
        finish_kernel,
        out_shape=(
            jax.ShapeDtypeStruct(tokens.shape, BF16),
            jax.ShapeDtypeStruct(states.shape, F32),
        ),
        in_specs=[anywhere] * 2,
        out_specs=(anywhere, anywhere),
        scratch_shapes=[dma((2,))],
        compiler_params=pltpu.CompilerParams(vmem_limit_bytes=1048576),
    )(result, fresh)


def dispatch(groups, halves, *arrays):
    rows, cols = arrays[0].shape
    if rows == 8 and cols % 128 == 0 and rows % groups == 0 and groups > 2 and halves <= 4:
        return fused(groups, halves, *arrays)
    return body(*arrays)


def solution(mesh):
    placed = (
        P("dp", ("kv", "tp")),
        P(None, "tp", "kv"),
        P(None, "tp", "kv"),
        P(None, "tp", "kv"),
        P(None, "tp", "kv"),
        P(None, "tp", "kv"),
        P("tp", None),
        P(("dp", "kv"), "tp", None, None),
        P("tp", None),
        P(None, ("kv", "tp")),
        P(("kv", "tp")),
        P(("kv", "tp")),
        P(None, ("kv", "tp")),
        P(("kv", "tp"), None),
        P(("kv", "tp")),
        P(("kv", "tp")),
    )
    return jax.shard_map(
        functools.partial(dispatch, mesh.shape["kv"], mesh.shape["tp"]),
        mesh=mesh,
        in_specs=placed,
        out_specs=(P("dp", ("kv", "tp")), P(("dp", "kv"), "tp", None, None)),
        check_vma=False,
    )
```
